32 devices in a mesh: grp: 2 (over y), fs: 4 (over z), tp: 4 (over x, core).
Axes of the slice: x: 2, y: 2, z: 4, core: 2. Of those that a mesh axis runs over, the one named last changes fastest.
Arguments:
- tokens: bfloat16 [4096, 2048], P(('grp', 'fs'), 'tp'), parts along dimension 0, may hold values from -16 to 16
- attn_gain: float32 [2048], replicated, may hold values from 0.1 to 1.9
- w_query: bfloat16 [2048, 1024], P('fs', 'tp'), may hold values from -0.125 to 0.125
- w_key: bfloat16 [2048, 1024], P('fs', 'tp'), may hold values from -0.125 to 0.125
- w_value: bfloat16 [2048, 2048], P('fs', 'tp'), may hold values from -0.125 to 0.125
- w_low: bfloat16 [2048, 32], replicated, may hold values from -0.125 to 0.125
- w_lift: bfloat16 [32, 1024], P(None, 'tp'), may hold values from -1 to 1
- decay_bias: float32 [1024], P('tp'), may hold values from -0.5 to 6
- head_gain: float32 [256], replicated, may hold values from 0.1 to 1.9
- w_out: bfloat16 [2048, 2048], P('tp', 'fs'), may hold values from -0.125 to 0.125
- ffn_gain: float32 [2048], replicated, may hold values from 0.1 to 1.9
- w_gate: bfloat16 [2048, 5632], P('fs', 'tp'), may hold values from -0.125 to 0.125
- w_up: bfloat16 [2048, 5632], P('fs', 'tp'), may hold values from -0.125 to 0.125
- w_down: bfloat16 [5632, 2048], P('tp', 'fs'), may hold values from -0.078125 to 0.078125
- final_gain: float32 [2048], P('tp'), may hold values from 0.1 to 1.9
Outputs:
- result: bfloat16 [4096, 2048], P(('grp', 'fs'), 'tp'), parts along dimension 0
The draws below stay inside these ranges and needn't reach their ends.
There are 2 independent parts, one for each index of `grp`. The reference program is written for one: setup_inputs(seed, part) draws one part's arguments, and reference() takes and returns one part's arrays. A program takes and returns all parts, laid end to end along the dimension named above; an argument that names none is the same for every part. Nothing has to cross between parts.
All inputs are finite; a program needn't handle non-finite values.
Results may differ from the reference program's by a relative error of at most 0.015.
Values may be sent and summed in bfloat16 or wider, within the bound.
A program may use at most 64 MiB of HBM per device.

```python
import math
import jax
import jax.numpy as jnp
from jax import lax

D = 2048
HEADS = 8
DK = 128
DV = 256
RANK = 32
FF = 5632
BLOCK = 64
LEN = 512
QK = 1024
V = 2048
TOKENS = 2048
N_FS = 4
N_TP = 4


def draw_tokens(key, part):
    first_key, second_key = jax.random.split(jax.random.fold_in(key, 11), 2)
    groups = 8
    scales = jnp.exp(jax.random.uniform(first_key, (groups,), jnp.float32, math.log(0.25), math.log(4.0)))
    scales = jnp.repeat(scales, D // groups)
    base = jnp.clip(jax.random.normal(second_key, (TOKENS, D), jnp.float32), -4.0, 4.0)
    return (base * scales[None, :]).astype(jnp.bfloat16)


def draw_decay_bias(key, part):
    first_key, second_key, third_key = jax.random.split(jax.random.fold_in(key, 23), 3)
    fast_share = 0.5
    is_fast = jax.random.uniform(first_key, (QK,), jnp.float32) < fast_share
    fast_value = jax.random.uniform(second_key, (QK,), jnp.float32, -0.5, 0.5)
    slow_value = jax.random.uniform(third_key, (QK,), jnp.float32, 4.5, 6.0)
    return jnp.where(is_fast, fast_value, slow_value)


def block_levels(stream_key, extent, shards, smallest, high):
    def one(axis_at, shards_of):
        heights = jax.random.uniform(jax.random.fold_in(jax.random.fold_in(stream_key, 6), axis_at), (shards_of,), jnp.float32, smallest / len(shards), high / len(shards))
        return jnp.repeat(jnp.exp(heights), extent[axis_at] // shards_of).reshape((-1,) + (1,) * (len(extent) - axis_at - 1))

    level = one(*shards[0])
    for cut in shards[1:]:
        level = level * one(*cut)
    return level


def noise(key, shape, width, bound, pieces=(), kind=jnp.bfloat16):
    values = width * jax.random.normal(key, shape, jnp.float32)
    if pieces:
        values = values * block_levels(key, shape, pieces, -0.22, 0.18)
    return jnp.clip(values, -bound, bound).astype(kind)


def setup_inputs(seed: int = 0, part: int = 0) -> dict:
    streams_of = jax.random.split(jax.random.key(seed), 16)
    own_keys = jax.random.split(jax.random.fold_in(streams_of[15], part), 16)
    return {
        "tokens": draw_tokens(jax.random.fold_in(jax.random.fold_in(streams_of[15], part), 71), part),
        "attn_gain": jnp.clip(1.0 + 0.18 * jax.random.normal(streams_of[1], (D,), jnp.float32), 0.1, 1.9),
        "w_query": noise(streams_of[2], (D, QK), D ** -0.5, 0.125, ((0, 4), (1, 4))),
        "w_key": noise(streams_of[3], (D, QK), D ** -0.5, 0.125, ((0, 4), (1, 4))),
        "w_value": noise(streams_of[4], (D, V), D ** -0.5, 0.125, ((0, 4), (1, 4))),
        "w_low": noise(streams_of[5], (D, RANK), D ** -0.5, 0.125),
        "w_lift": noise(streams_of[6], (RANK, QK), RANK ** -0.5, 1.0, ((1, 4),)),
        "decay_bias": draw_decay_bias(jax.random.fold_in(streams_of[15], 71), part),
        "head_gain": jnp.clip(1.0 + 0.18 * jax.random.normal(streams_of[8], (DV,), jnp.float32), 0.1, 1.9),
        "w_out": noise(streams_of[9], (V, D), V ** -0.5, 0.125, ((0, 4), (1, 4))),
        "ffn_gain": jnp.clip(1.0 + 0.18 * jax.random.normal(streams_of[10], (D,), jnp.float32), 0.1, 1.9),
        "w_gate": noise(streams_of[11], (D, FF), D ** -0.5, 0.125, ((0, 4), (1, 4))),
        "w_up": noise(streams_of[12], (D, FF), D ** -0.5, 0.125, ((0, 4), (1, 4))),
        "w_down": noise(streams_of[13], (FF, D), FF ** -0.5, 0.078125, ((0, 4), (1, 4))),
        "final_gain": jnp.clip(1.0 + 0.18 * jax.random.normal(streams_of[14], (D,), jnp.float32), 0.1, 1.9),
    }


epsilon = 1e-06
highest = lax.Precision.HIGHEST

def rms_rows(values, gain):
    values = values.astype(jnp.float32)
    factor = lax.rsqrt(lax.optimization_barrier(jnp.mean(values * values, axis=-1, keepdims=True)) + epsilon)
    return values * factor * gain.astype(jnp.float32)

def blockwise_gla(query_rows, key_rows, value_rows, log_decay, head_count):
    length = query_rows.shape[0]
    blocks = length // BLOCK

    def split_heads(array, depth):
        return array.astype(jnp.float32).reshape(blocks, BLOCK, head_count, depth).transpose(2, 0, 1, 3)
    query_f = split_heads(query_rows, DK) * DK ** (-0.5)
    key_f = split_heads(key_rows, DK)
    value_f = split_heads(value_rows, DV)
    log_cum = jnp.cumsum(split_heads(log_decay, DK), axis=2)
    log_last = log_cum[:, :, -1:, :]
    query_dec = query_f * jnp.exp(log_cum)
    key_dec = key_f * jnp.exp(-log_cum)
    causal = jnp.tril(jnp.ones((BLOCK, BLOCK), dtype=bool))
    scores = jnp.where(causal, jnp.einsum('hncd,hnsd->hncs', query_dec, key_dec, precision=highest), 0.0)
    inside = jnp.einsum('hncs,hnsv->hncv', scores, value_f, precision=highest)
    contrib = jnp.einsum('hncd,hncv->hndv', key_f * jnp.exp(log_last - log_cum), value_f, precision=highest)
    decay_block = jnp.exp(log_last[:, :, 0, :])

    def advance(carry_state, inputs):
        decay_step, added = inputs
        return (decay_step[..., None] * carry_state + added, carry_state)
    start_state = jnp.zeros((head_count, DK, DV), jnp.float32)
    final_state, earlier = lax.scan(advance, start_state, (jnp.moveaxis(decay_block, 1, 0), jnp.moveaxis(contrib, 1, 0)))
    earlier = jnp.moveaxis(earlier, 0, 1)
    output = inside + jnp.einsum('hncd,hndv->hncv', query_dec, earlier, precision=highest)
    return output.transpose(1, 2, 0, 3).reshape(length, head_count, DV)

def reference(tokens, attn_gain, w_query, w_key, w_value, w_low, w_lift, decay_bias, head_gain, w_out, ffn_gain, w_gate, w_up, w_down, final_gain):
    normed = rms_rows(tokens, attn_gain).astype(jnp.bfloat16)
    query_rows = jnp.dot(normed, w_query, preferred_element_type=jnp.float32).astype(jnp.bfloat16)
    key_rows = jnp.dot(normed, w_key, preferred_element_type=jnp.float32).astype(jnp.bfloat16)
    value_rows = jnp.dot(normed, w_value, preferred_element_type=jnp.float32).astype(jnp.bfloat16)
    low_rank = jnp.dot(normed, w_low, preferred_element_type=jnp.float32).astype(jnp.bfloat16)
    log_decay = jax.nn.log_sigmoid(jnp.dot(low_rank, w_lift, preferred_element_type=jnp.float32) + decay_bias.astype(jnp.float32)) / 16.0
    gla_out = jax.vmap(lambda qq, kk, vv, gg: blockwise_gla(qq, kk, vv, gg, HEADS))(query_rows.reshape(N_FS, LEN, QK), key_rows.reshape(N_FS, LEN, QK), value_rows.reshape(N_FS, LEN, V), log_decay.reshape(N_FS, LEN, QK))
    gla_out = gla_out.reshape(TOKENS, HEADS, DV)
    mixed_heads = rms_rows(gla_out, head_gain).reshape(TOKENS, V).astype(jnp.bfloat16)
    span = V // N_TP
    attn_sum = jnp.zeros((TOKENS, D), jnp.float32)
    for index in range(N_TP):
        partial_prod = jnp.dot(mixed_heads[:, index * span:(index + 1) * span], w_out[index * span:(index + 1) * span], preferred_element_type=jnp.float32).astype(jnp.bfloat16)
        attn_sum = attn_sum + partial_prod.astype(jnp.float32)
    first_sum = (tokens.astype(jnp.float32) + attn_sum).astype(jnp.bfloat16)
    normed_ffn = rms_rows(first_sum, ffn_gain).astype(jnp.bfloat16)
    gate_rows = jnp.dot(normed_ffn, w_gate, preferred_element_type=jnp.float32)
    up_rows = jnp.dot(normed_ffn, w_up, preferred_element_type=jnp.float32)
    hidden = (jax.nn.silu(gate_rows) * up_rows).astype(jnp.bfloat16)
    units = FF // N_TP
    ffn_sum = jnp.zeros((TOKENS, D), jnp.float32)
    for index in range(N_TP):
        partial_prod = jnp.dot(hidden[:, index * units:(index + 1) * units], w_down[index * units:(index + 1) * units], preferred_element_type=jnp.float32).astype(jnp.bfloat16)
        ffn_sum = ffn_sum + partial_prod.astype(jnp.float32)
    second_sum = first_sum.astype(jnp.float32) + ffn_sum
    return rms_rows(second_sum, final_gain).astype(jnp.bfloat16)
```

```python
import functools

import jax
import jax.numpy as jnp
from jax import lax
from jax.experimental import pallas as pl
from jax.experimental.pallas import tpu as pltpu
from jax.sharding import PartitionSpec as P

DK = 128
DV = 256
BLOCK = 64
epsilon = 1e-06
highest = lax.Precision.HIGHEST
MESH = pl.DeviceIdType.MESH
LANES = 128
HALVES = 2


def unit_chunks(units):
    if units % LANES:
        return [(0, units)]
    tiles = units // LANES
    pieces = [-(-tiles // 3) + (-(-tiles // 3)) % 2] * 3
    chunks, start = [], 0
    for piece in pieces:
        size = min(piece, tiles - start)
        if size > 0:
            chunks.append((start * LANES, size * LANES))
            start += size
    return chunks


def down_columns(columns):
    return 2 * LANES if columns % (2 * LANES) == 0 else LANES


def layer_kernel(
    sizes,
    tokens_ref,
    attn_gain_ref,
    w_low_ref,
    w_lift_ref,
    decay_bias_ref,
    head_gain_ref,
    ffn_gain_ref,
    final_gain_ref,
    w_query_ref,
    w_key_ref,
    w_value_ref,
    w_out_ref,
    w_gate_ref,
    w_up_ref,
    w_down_ref,
    result_ref,
    g_mix,
    g_out,
    g_gate,
    g_up,
    g_down,
    rows_all,
    normed,
    mix_rows,
    log_decay,
    mixed,
    state,
    partial_out,
    sib_out,
    far_out,
    first_all,
    hidden,
    partial_down,
    sib_down,
    far_down,
    sum_out,
    sum_in,
    second,
    squares,
    z_send,
    z_recv,
    y_send,
    y_recv,
    e_send,
    e_recv,
    ag_send,
    ag_recv,
    rs_send,
    rs_recv,
    dd_send,
    dd_recv,
    dx_send,
    dx_recv,
    guest_send,
    guest_recv,
    back_send,
    back_recv,
    sq_send,
    sq_recv,
    local_sem,
):
    n, tp = sizes
    chips = tp // 2
    g, f, t = lax.axis_index("grp"), lax.axis_index("fs"), lax.axis_index("tp")
    chip, core = t // 2, lax.rem(t, 2)
    sibling = t + 1 - 2 * core
    rows, width = tokens_ref.shape
    features = width * tp
    f32, bf16 = jnp.float32, jnp.bfloat16
    inner = jnp.logical_and(f > 0, f < n - 1)
    outer = jnp.logical_not(inner)
    has_guest = jnp.logical_or(f == 1, f == n - 2)
    guests = jnp.where(has_guest, 1, 0)
    guest_plane = jnp.where(f == 1, 0, n - 1)
    host_plane = jnp.where(f == 0, 1, n - 2)
    near = jnp.where(2 * f < n, 0, 1)
    far = 1 - near

    messages = []
    column = 0
    for w in (w_query_ref, w_key_ref, w_value_ref):
        messages.append((w, g_mix, 0, column, w.shape[1]))
        column += w.shape[1]
    messages.append((w_out_ref, g_out, 0, 0, w_out_ref.shape[1]))
    n_mix = len(messages)
    qkv, outs = range(3), range(3, 4)
    chunks = unit_chunks(w_gate_ref.shape[1])
    ffn_groups = []
    for start, size in chunks:
        ffn_groups.append((len(messages), len(messages) + 1))
        messages.append((w_gate_ref, g_gate, start, start, size))
        messages.append((w_up_ref, g_up, start, start, size))
    cols = w_down_ref.shape[1]
    dc = down_columns(cols)
    pieces = cols // dc
    down_at = len(messages)
    for c in range(pieces):
        messages.append((w_down_ref, g_down, c * dc, c * dc, dc))
    down_groups = [(down_at + c,) for c in range(pieces)]
    total_messages = len(messages)

    def is_ffn(m):
        return m >= n_mix

    def comes_whole(m, step):
        return step == 1 and (is_ffn(m) or m in qkv)

    def steps_of(m):
        return n - 2 if is_ffn(m) else n - 1

    barrier = pltpu.get_barrier_semaphore()

    @pl.when(f > 0)
    def _():
        pl.semaphore_signal(barrier, inc=1, device_id=(g, f - 1, t), device_id_type=MESH)

    @pl.when(f < n - 1)
    def _():
        pl.semaphore_signal(barrier, inc=1, device_id=(g, f + 1, t), device_id_type=MESH)

    pl.semaphore_signal(barrier, inc=1, device_id=(1 - g, f, t), device_id_type=MESH)
    for d in range(1, tp):
        peer = lax.rem(t + d, tp)
        pl.semaphore_signal(barrier, inc=1, device_id=(g, f, peer), device_id_type=MESH)
    met = jnp.where(f > 0, 1, 0) + jnp.where(f < n - 1, 1, 0) + tp
    pl.semaphore_wait(barrier, met)

    def half_of(w, which):
        part = w.shape[0] // 2
        return pl.ds(pl.multiple_of(which * part, 16), part)

    def toward(way):
        return f + 1 - 2 * way

    def z_copy(m, way, step):
        w, held, start, column, columns = messages[m]
        owner = f + (step - 1) * (2 * way - 1)
        half = half_of(w, g)
        at = held.at[owner, half, pl.ds(column, columns)]
        source = w.at[half, pl.ds(start, columns)] if step == 1 else at
        return pltpu.make_async_remote_copy(
            source, at, z_send.at[m, way, step], z_recv.at[m, way, step],
            device_id=(g, toward(way), t), device_id_type=MESH,
        )

    def e_copy(m, way, owner):
        w, held, start, column, columns = messages[m]
        half = half_of(w, 1 - g)
        at = held.at[owner, half, pl.ds(column, columns)]
        return pltpu.make_async_remote_copy(
            w.at[half, pl.ds(start, columns)], at, e_send.at[m, way], e_recv.at[m, way],
            device_id=(g, toward(way), t), device_id_type=MESH,
        )

    def y_copy(m, way, step):
        w, held, _, column, columns = messages[m]
        at = held.at[f + step * (2 * way - 1), half_of(w, g), pl.ds(column, columns)]
        return pltpu.make_async_remote_copy(
            at, at, y_send.at[m, way, step], y_recv.at[m, way, step],
            device_id=(1 - g, f, t), device_id_type=MESH,
        )

    def gets(m, way, step):
        j = f + step * (2 * way - 1)
        there = jnp.logical_and(j >= 0, j < n)
        return jnp.logical_and(there, inner) if is_ffn(m) else there

    def gives(m, way, step):
        j = f + (step - 1) * (2 * way - 1)
        there = jnp.logical_and(j >= 0, j < n)
        to = toward(way)
        low, high = (1, n - 2) if is_ffn(m) else (0, n - 1)
        return jnp.logical_and(there, jnp.logical_and(to >= low, to <= high))

    def gives_whole(way):
        return f == jnp.where(way == 0, 0, n - 1)

    def gets_whole(way):
        return f == jnp.where(way == 0, 1, n - 2)

    def launch(group, way):
        for m in group:
            @pl.when(gives(m, way, 1))
            def _():
                z_copy(m, way, 1).start()

    def complete(group):
        for way in (0, 1):
            for m in group:
                @pl.when(gives_whole(way))
                def _():
                    e_copy(m, way, f).start()

    def tick(group, way, step):
        for m in group:
            if step > steps_of(m):
                continue

            @pl.when(gets(m, way, step))
            def _():
                received(m, way, step).wait_recv()
                if comes_whole(m, step):
                    @pl.when(jnp.logical_not(gets_whole(way)))
                    def _():
                        y_copy(m, way, step).start()
                else:
                    y_copy(m, way, step).start()

            if step < steps_of(m):
                @pl.when(gives(m, way, step + 1))
                def _():
                    z_copy(m, way, step + 1).start()

    def received(m, way, step):
        w, held, start, column, columns = messages[m]
        at = held.at[f + step * (2 * way - 1), half_of(w, g), pl.ds(column, columns)]
        return pltpu.make_async_remote_copy(
            at, at, z_send.at[m, way, step], z_recv.at[m, way, step],
            device_id=(g, toward(way), t), device_id_type=MESH,
        )

    def arrived(m, way, step):
        if comes_whole(m, step):
            whole = gets_whole(way)

            @pl.when(whole)
            def _():
                e_copy(m, way, f + 2 * way - 1).wait_recv()

            @pl.when(jnp.logical_not(whole))
            def _():
                y_copy(m, way, step).wait_recv()
        else:
            y_copy(m, way, step).wait_recv()

    def all_arrived(group):
        for m in group:
            for step in range(1, steps_of(m) + 1):
                for way in (0, 1):
                    @pl.when(gets(m, way, step))
                    def _():
                        arrived(m, way, step)

    def peer_of(e):
        return 2 * lax.rem(chip + e, chips) + core

    def from_of(e):
        return 2 * lax.rem(chip - e + chips, chips) + core

    def tp_copy(source, target, send, recv, peer):
        return pltpu.make_async_remote_copy(
            source, target, send, recv, device_id=(g, f, peer), device_id_type=MESH
        )

    def ag_copy(kind, slot, source, target, peer):
        return tp_copy(source, target, ag_send.at[kind, slot], ag_recv.at[kind, slot], peer)

    others = range(1, tp)
    beyond = range(1, chips)

    def gather_out(kind, source, at):
        for e in beyond:
            ag_copy(kind, e, source, at(t), peer_of(e)).start()
        ag_copy(kind, 0, source, at(t), sibling).start()

    def gather_forward(kind, at):
        for e in beyond:
            came = at(from_of(e))
            ag_copy(kind, e, came, came, peer_of(e)).wait_recv()
            ag_copy(kind, chips - 1 + e, came, came, sibling).start()

    def gather_wait(kind, at):
        ag_copy(kind, 0, at(sibling), at(sibling), sibling).wait_recv()
        for e in beyond:
            came = at(from_of(e) + 1 - 2 * core)
            ag_copy(kind, chips - 1 + e, came, came, sibling).wait_recv()

    def gather_drain(kind, at):
        for slot in range(tp - 1):
            ag_copy(kind, slot, at(t), at(t), sibling).wait_send()

    def rows_of(h):
        return pl.ds(h * (rows // HALVES), rows // HALVES)

    def token_at(p):
        return rows_all.at[p]

    def first_at(r, h):
        return lambda p: first_all.at[r, p, rows_of(h)]

    def ag_kind(r, h):
        return 1 + r * HALVES + h

    def square_copy(d):
        peer = lax.rem(t + d, tp)
        return tp_copy(squares.at[0], squares.at[d], sq_send.at[d], sq_recv.at[d], peer)

    ahead = ffn_groups + down_groups
    ways = {"near": (near, n // 2 - 1), "far": (far, n - 2)}
    launched, ticked = set(), set()

    def send_own(i):
        if i < len(ahead) and i not in launched:
            launched.add(i)
            for way in (0, 1):
                launch(ahead[i], way)

    def relay(i, which, step=None):
        if i >= len(ahead):
            return
        way, top = ways[which]
        for s in range(1, top + 1):
            if step in (None, s) and (i, which, s) not in ticked:
                ticked.add((i, which, s))
                tick(ahead[i], way, s)

    def relayed(i):
        send_own(i)
        relay(i, "near")
        relay(i, "far")

    first_down = len(ffn_groups)

    def pump(k):
        for act in plan.get(k, ()):
            act()

    last_unit = len(ffn_groups) - 1
    plan = {
        -1: [lambda: send_own(0), lambda: send_own(1)],
        0: [lambda: relay(0, "near")],
        1: [lambda: relay(0, "far", 1)],
        2: [lambda: send_own(2), lambda: relay(1, "far", 1)],
        3: [lambda: relay(1, "near"), lambda: relay(0, "far"), lambda: send_own(3)],
        4: [lambda: relay(2, "far", 1)],
        5: [lambda: relay(2, "near"), lambda: send_own(4), lambda: relay(1, "far")],
        6: [lambda: relay(3, "far", 1)],
        7: [lambda: relay(2, "far")],
        8: [lambda: relay(4, "far", 1), lambda: relay(3, "near")],
        9: [lambda: relay(3, "far")],
        10: [lambda: relay(4, "near")],
    }

    def last_step(way):
        return jnp.where(way == 0, f, n - 1 - f)

    def after(step, way, group):
        @pl.when(last_step(way) == step)
        def _():
            launch(group, way)

    for way in (0, 1):
        launch(qkv, way)
        after(0, way, outs)

    @pl.when(outer)
    def _():
        complete(qkv)
        for group in ffn_groups:
            for way in (0, 1):
                launch(group, way)
            if group != ffn_groups[-1]:
                complete(group)

    gather_out(0, tokens_ref, token_at)
    locals_ = [pltpu.make_async_copy(tokens_ref, rows_all.at[t], local_sem.at[0])]
    own = [messages[m] for m in range(n_mix)]
    for index, (w, held, start, column, columns) in enumerate(own):
        at = held.at[f, :, pl.ds(column, columns)]
        locals_.append(pltpu.make_async_copy(w, at, local_sem.at[1 + index]))
    inner_locals = []
    for index, (w, held) in enumerate(((w_gate_ref, g_gate), (w_up_ref, g_up), (w_down_ref, g_down))):
        inner_locals.append(pltpu.make_async_copy(w, held.at[f], local_sem.at[1 + n_mix + index]))
    for copy in locals_:
        copy.start()

    @pl.when(inner)
    def _():
        for copy in inner_locals:
            copy.start()

    for step in range(1, n):
        for m in qkv:
            for way in (0, 1):
                tick((m,), way, step)
        for way in (0, 1):
            after(step, way, outs)
        if step == 1:
            gather_forward(0, token_at)
    for step in range(1, n // 2):
        tick(outs, near, step)
    pl.when(inner)(lambda: pump(-1))

    @pl.when(inner)
    def _():
        for copy in inner_locals:
            copy.wait()

    for copy in locals_:
        copy.wait()
    gather_wait(0, token_at)

    def normalize(source, slot, gain_ref, at):
        total = jnp.zeros((at.size, 1), f32)
        for p in range(tp):
            values = source[p, at].astype(f32)
            total += jnp.sum(values * values, axis=1, keepdims=True)
        factor = lax.rsqrt(total / features + epsilon)
        for p in range(tp):
            part = pl.ds(p * width, width)
            scaled = source[p, at].astype(f32) * factor * gain_ref[:, part]
            normed[slot, at, part] = scaled.astype(bf16)

    def product(lhs, held, at, size):
        block = held[:, :, pl.ds(at, size)]
        block = block.reshape(block.shape[0] * block.shape[1], size)
        return jnp.dot(lhs, block, preferred_element_type=f32)

    for h in range(HALVES):
        normalize(rows_all, 0, attn_gain_ref, rows_of(h))
    low_rank = lax.dot_general(
        normed[0], w_low_ref[...], (((1,), (1,)), ((), ())), preferred_element_type=f32
    )
    lifted = jnp.dot(low_rank.astype(bf16), w_lift_ref[...], preferred_element_type=f32)
    log_decay[...] = jax.nn.log_sigmoid(lifted + decay_bias_ref[...]) / 16.0

    all_arrived(qkv)
    tick(outs, far, 1)
    mix_block = 2 * LANES if mix_rows.shape[1] % (2 * LANES) == 0 else LANES

    def mix_step(i, carry):
        at = pl.multiple_of(i * mix_block, LANES)
        mix_rows[:, pl.ds(at, mix_block)] = product(normed[0], g_mix, at, mix_block).astype(bf16)
        return carry

    lax.fori_loop(0, mix_rows.shape[1] // mix_block, mix_step, 0)
    for step in range(2, n - 1):
        tick(outs, far, step)

    pl.when(inner)(lambda: pump(0))
    heads = mix_rows.shape[1] // (2 * DK + DV)
    at_row = lax.broadcasted_iota(jnp.int32, (BLOCK, BLOCK), 0)
    at_col = lax.broadcasted_iota(jnp.int32, (BLOCK, BLOCK), 1)
    causal = at_row >= at_col
    lower = causal.astype(f32)

    def dot(a, b, ca, cb):
        return lax.dot_general(
            a, b, (((ca,), (cb,)), ((), ())), precision=highest, preferred_element_type=f32
        )

    state[...] = jnp.zeros_like(state)

    def block_step(block, carry):
        here = pl.ds(pl.multiple_of(block * BLOCK, BLOCK), BLOCK)
        for h in range(heads):
            query = mix_rows[here, pl.ds(h * DK, DK)].astype(f32) * DK ** (-0.5)
            key = mix_rows[here, pl.ds((heads + h) * DK, DK)].astype(f32)
            value = mix_rows[here, pl.ds(2 * heads * DK + h * DV, DV)].astype(f32)
            cum = dot(lower, log_decay[here, pl.ds(h * DK, DK)], 1, 0)
            last = cum[BLOCK - 1 :, :]
            query_dec = query * jnp.exp(cum)
            key_dec = key * jnp.exp(-cum)
            scores = jnp.where(causal, dot(query_dec, key_dec, 1, 1), 0.0)
            held = state[h]
            out = dot(scores, value, 1, 0) + dot(query_dec, held, 1, 0)
            decay = jnp.transpose(jnp.broadcast_to(jnp.exp(last), (DK, DK)))
            decay = jnp.concatenate([decay] * (DV // DK), axis=1)
            state[h] = decay * held + dot(key * jnp.exp(last - cum), value, 0, 0)
            factor = lax.rsqrt(jnp.mean(out * out, axis=1, keepdims=True) + epsilon)
            mixed[here, pl.ds(h * DV, DV)] = (out * factor * head_gain_ref[...]).astype(bf16)
        return carry

    blocks = rows // BLOCK
    lax.fori_loop(0, blocks // 2, block_step, 0)
    pl.when(inner)(lambda: pump(1))
    lax.fori_loop(blocks // 2, blocks, block_step, 0)
    tick(outs, far, n - 1)
    all_arrived(outs)

    def block_place(place, size):
        return place // width, pl.ds(pl.multiple_of(lax.rem(place, width), LANES), size)

    def rs_copy(h, slot, source, target, peer):
        return tp_copy(source, target, rs_send.at[h, slot], rs_recv.at[h, slot], peer)

    def sib_copy(h, c):
        return rs_copy(
            h, c, partial_out.at[2 * c + 1 - core, rows_of(h)], sib_out.at[c, rows_of(h)], sibling
        )

    def far_copy(h, e):
        return rs_copy(
            h, chips - 1 + e, partial_out.at[peer_of(e), rows_of(h)],
            far_out.at[e - 1, rows_of(h)], peer_of(e),
        )

    out_cols = g_out.shape[2]
    for h in range(HALVES):
        def out_step(j, carry):
            p, part = block_place(j * out_cols, out_cols)
            terms = jnp.dot(mixed[rows_of(h), :], g_out[j], preferred_element_type=f32)
            partial_out[p, rows_of(h), part] = terms.astype(bf16)
            return carry

        lax.fori_loop(0, n, out_step, 0)
        for c in range(chips):
            sib_copy(h, c).start()
    for h in range(HALVES):
        for c in range(chips):
            sib_copy(h, c).wait_recv()
        for e in beyond:
            there = lax.rem(chip + e, chips)
            p = peer_of(e)
            pair = partial_out[p, rows_of(h)].astype(f32) + sib_out[there, rows_of(h)].astype(f32)
            partial_out[p, rows_of(h)] = pair.astype(bf16)
            far_copy(h, e).start()
    pl.when(inner)(lambda: pump(2))

    def guest_copy(h):
        at = rows_of(h)
        return pltpu.make_async_remote_copy(
            first_all.at[0, t, at], first_all.at[1, t, at], guest_send.at[h], guest_recv.at[h],
            device_id=(g, host_plane, t), device_id_type=MESH,
        )

    for h in range(HALVES):
        for e in beyond:
            far_copy(h, e).wait_recv()
        total = partial_out[t, rows_of(h)].astype(f32) + sib_out[chip, rows_of(h)].astype(f32)
        for e in beyond:
            total += far_out[e - 1, rows_of(h)].astype(f32)
        first_all[0, t, rows_of(h)] = (rows_all[t, rows_of(h)].astype(f32) + total).astype(bf16)

        @pl.when(inner)
        def _():
            gather_out(ag_kind(0, h), first_all.at[0, t, rows_of(h)], first_at(0, h))

        @pl.when(outer)
        def _():
            guest_copy(h).start()

    @pl.when(outer)
    def _():
        complete(ffn_groups[-1])
        for way in (0, 1):
            for group in down_groups:
                launch(group, way)
        for group in down_groups:
            complete(group)

    def units_step(r, start, size):
        gate = product(normed[r], g_gate, start, size)
        up = product(normed[r], g_up, start, size)
        hidden[r, :, pl.ds(start, size)] = (gate / (1.0 + jnp.exp(-gate)) * up).astype(bf16)

    def ffn_chunk(ci, r):
        start, size = chunks[ci]
        block = 2 * LANES
        whole = size // block

        def step(i, carry):
            units_step(r, pl.multiple_of(start + i * block, LANES), block)
            return carry

        lax.fori_loop(0, whole, step, 0)
        if size % block:
            units_step(r, start + whole * block, size % block)

    def guest_gather():
        for h in range(HALVES):
            guest_copy(h).wait_recv()
            gather_out(ag_kind(1, h), first_all.at[1, t, rows_of(h)], first_at(1, h))

    def guest_forward():
        for h in range(HALVES):
            gather_forward(ag_kind(1, h), first_at(1, h))

    def guest_ready():
        for h in range(HALVES):
            gather_wait(ag_kind(1, h), first_at(1, h))
            normalize(first_all.at[1], 1, ffn_gain_ref, rows_of(h))

    def place_of(j, c):
        p, part = block_place(j * cols + c * dc, dc)
        return p, part

    def dd_copy(r, j, c):
        p, part = place_of(j, c)
        return tp_copy(
            partial_down.at[r, p, :, part], sib_down.at[r, p // 2, :, part],
            dd_send.at[j * pieces + c, r], dd_recv.at[j * pieces + c, r], sibling,
        )

    def dx_copy(r, j, c, e):
        p, part = place_of(j, c)
        return tp_copy(
            partial_down.at[r, p, :, part], far_down.at[r, e - 1, :, part],
            dx_send.at[j * pieces + c, r, e - 1], dx_recv.at[j * pieces + c, r, e - 1],
            2 * (p // 2) + core,
        )

    def sets(act):
        def one(i, carry):
            act(guests - i)
            return carry

        lax.fori_loop(0, 1 + guests, one, 0)

    def down_compute(j, c):
        p, part = place_of(j, c)

        def act(r):
            terms = jnp.dot(hidden[r], g_down[j, :, pl.ds(c * dc, dc)], preferred_element_type=f32)
            partial_down[r, p, :, part] = terms.astype(bf16)

            @pl.when(lax.rem(p, 2) != core)
            def _():
                dd_copy(r, j, c).start()

        sets(act)

    def down_pass(j, c):
        p, part = place_of(j, c)

        @pl.when(jnp.logical_and(lax.rem(p, 2) == core, p // 2 != chip))
        def _():
            def act(r):
                dd_copy(r, j, c).wait_recv()
                pair = partial_down[r, p, :, part].astype(f32)
                pair += sib_down[r, p // 2, :, part].astype(f32)
                partial_down[r, p, :, part] = pair.astype(bf16)
                for e in beyond:
                    @pl.when(lax.rem(chip + e, chips) == p // 2)
                    def _():
                        dx_copy(r, j, c, e).start()

            sets(act)

    def down_total(r):
        for j in range(n):
            for c in range(pieces):
                @pl.when((j * cols + c * dc) // width == t)
                def _():
                    dd_copy(r, j, c).wait_recv()
                    for e in beyond:
                        dx_copy(r, j, c, e).wait_recv()
        total = partial_down[r, t].astype(f32) + sib_down[r, chip].astype(f32)
        for e in beyond:
            total += far_down[r, e - 1].astype(f32)
        return total

    def back_copy():
        return pltpu.make_async_remote_copy(
            sum_out, sum_in, back_send, back_recv,
            device_id=(g, guest_plane, t), device_id_type=MESH,
        )

    @pl.when(inner)
    def _():
        pump(3)
        for h in range(HALVES):
            gather_forward(ag_kind(0, h), first_at(0, h))
        for h in range(HALVES):
            gather_wait(ag_kind(0, h), first_at(0, h))
            normalize(first_all.at[0], 0, ffn_gain_ref, rows_of(h))
        pump(4)
        last = len(chunks) - 1
        for ci in range(max(1, last)):
            relayed(ci)
            all_arrived(ffn_groups[ci])
            if ci == min(1, last):
                pl.when(has_guest)(guest_gather)
                pump(6)
            ffn_chunk(ci, 0)
            if ci == 0:
                pump(5)
        pl.when(has_guest)(guest_forward)
        pump(7)
        pl.when(has_guest)(guest_ready)
        for ci in range(max(1, last)):
            pl.when(has_guest)(lambda: ffn_chunk(ci, 1))
            if ci == 0:
                pump(8)
        if last > 0:
            relayed(last)
            all_arrived(ffn_groups[last])
            ffn_chunk(last, 0)
            pump(9)
            pl.when(has_guest)(lambda: ffn_chunk(last, 1))
        pump(10)
        for i in range(len(ahead)):
            send_own(i)
        waiting = []

        def entry(valid, j, c, ready, hurry):
            @pl.when(valid)
            def _():
                ready()
                down_compute(j, c)

            if waiting:
                settle()
            waiting.append((valid, j, c))
            if hurry:
                settle()

        def settle():
            valid, j, c = waiting.pop()

            @pl.when(valid)
            def _():
                down_pass(j, c)

        for c in range(pieces):
            entry(True, f, c, lambda: None, False)
        for which in ("near", "far"):
            way, top = ways[which]
            for c in range(pieces):
                for step in range(1, top + 1):
                    m = down_at + c
                    relay(first_down + c, which, step)
                    ready = functools.partial(arrived, m, way, step)
                    j = f + step * (2 * way - 1)
                    entry(gets(m, way, step), j, c, ready, which == "far")
        if waiting:
            settle()

        @pl.when(has_guest)
        def _():
            sum_out[...] = down_total(1).astype(bf16)
            back_copy().start()

        second[...] = first_all[0, t].astype(f32) + down_total(0)

    @pl.when(outer)
    def _():
        back_copy().wait_recv()
        second[...] = first_all[0, t].astype(f32) + sum_in[...].astype(f32)

    ones = jnp.ones((8, width), f32)
    squares[0] = dot(ones, second[...] * second[...], 1, 1)
    for d in others:
        square_copy(d).start()
    for d in others:
        square_copy(d).wait_recv()
    whole = squares[0]
    for d in others:
        whole += squares[d]
    factor = lax.rsqrt(jnp.transpose(whole) / features + epsilon)[:, :1]
    result_ref[...] = (second[...] * factor * final_gain_ref[...]).astype(bf16)

    for m in range(total_messages):
        for step in range(1, steps_of(m) + 1):
            for way in (0, 1):
                @pl.when(gives(m, way, step))
                def _():
                    z_copy(m, way, step).wait_send()

                got = gets(m, way, step)
                if comes_whole(m, step):
                    got = jnp.logical_and(got, jnp.logical_not(gets_whole(way)))

                @pl.when(got)
                def _():
                    y_copy(m, way, step).wait_send()

                if comes_whole(m, step):
                    @pl.when(gives_whole(way))
                    def _():
                        e_copy(m, way, f).wait_send()
    gather_drain(0, token_at)
    for h in range(HALVES):
        for c in range(chips):
            sib_copy(h, c).wait_send()
        for e in beyond:
            far_copy(h, e).wait_send()
    for d in others:
        square_copy(d).wait_send()

    @pl.when(outer)
    def _():
        for h in range(HALVES):
            guest_copy(h).wait_send()

    def drain_down(r):
        for h in range(HALVES):
            gather_drain(ag_kind(r, h), first_at(r, h))
        for j in range(n):
            for c in range(pieces):
                p = (j * cols + c * dc) // width

                @pl.when(p % 2 != core)
                def _():
                    dd_copy(r, j, c).wait_send()

                for e in beyond:
                    @pl.when(jnp.logical_and(p % 2 == core, lax.rem(chip + e, chips) == p // 2))
                    def _():
                        dx_copy(r, j, c, e).wait_send()

    pl.when(inner)(lambda: drain_down(0))

    @pl.when(has_guest)
    def _():
        drain_down(1)
        back_copy().wait_send()


def body(
    sizes, tokens, attn_gain, w_query, w_key, w_value, w_low, w_lift, decay_bias, head_gain,
    w_out, ffn_gain, w_gate, w_up, w_down, final_gain,
):
    n, tp = sizes
    rows, width = tokens.shape
    bf16, f32 = jnp.bfloat16, jnp.float32
    units, keys, values = w_gate.shape[1], w_query.shape[1], w_value.shape[1]
    mix_width = 2 * keys + values
    chips = tp // 2
    vmem = pltpu.VMEM
    held = [vmem((n, w_query.shape[0], mix_width), bf16)]
    held += [vmem((n, *w.shape), bf16) for w in (w_out, w_gate, w_up, w_down)]
    pieces = w_down.shape[1] // down_columns(w_down.shape[1])
    messages = 4 + 2 * len(unit_chunks(units)) + pieces
    dma = pltpu.SemaphoreType.DMA
    anywhere = pl.BlockSpec(memory_space=pl.ANY)
    inside = pl.BlockSpec(memory_space=pltpu.VMEM)
    return pl.pallas_call(
        functools.partial(layer_kernel, sizes),
        name="layer",
        out_shape=jax.ShapeDtypeStruct((rows, width), bf16),
        in_specs=[anywhere] + [inside] * 7 + [anywhere] * 7,
        out_specs=inside,
        scratch_shapes=held + [
            vmem((tp, rows, width), bf16),
            vmem((2, rows, width * tp), bf16),
            vmem((rows, mix_width), bf16),
            vmem((rows, keys), f32),
            vmem((rows, values), bf16),
            vmem((keys // DK, DK, DV), f32),
            vmem((tp, rows, width), bf16),
            vmem((chips, rows, width), bf16),
            vmem((chips - 1, rows, width), bf16),
            vmem((2, tp, rows, width), bf16),
            vmem((2, rows, units), bf16),
            vmem((2, tp, rows, width), bf16),
            vmem((2, chips, rows, width), bf16),
            vmem((2, chips - 1, rows, width), bf16),
            vmem((rows, width), bf16),
            vmem((rows, width), bf16),
            vmem((rows, width), f32),
            vmem((tp, 8, rows), f32),
            dma((messages, 2, n)),
            dma((messages, 2, n)),
            dma((messages, 2, n)),
            dma((messages, 2, n)),
            dma((messages, 2)),
            dma((messages, 2)),
            dma((1 + 2 * HALVES, tp - 1)),
            dma((1 + 2 * HALVES, tp - 1)),
            dma((HALVES, tp - 1)),
            dma((HALVES, tp - 1)),
            dma((n * pieces, 2)),
            dma((n * pieces, 2)),
            dma((n * pieces, 2, chips - 1)),
            dma((n * pieces, 2, chips - 1)),
            dma((HALVES,)),
            dma((HALVES,)),
            dma,
            dma,
            dma((tp,)),
            dma((tp,)),
            dma((8,)),
        ],
        compiler_params=pltpu.CompilerParams(
            collective_id=0, has_side_effects=True, vmem_limit_bytes=63 * 1024 * 1024
        ),
    )(
        tokens, attn_gain[None], w_low.T, w_lift, decay_bias[None], head_gain[None],
        ffn_gain[None], final_gain[None], w_query, w_key, w_value, w_out, w_gate, w_up, w_down,
    )


def solution(mesh):
    sizes = (mesh.shape["fs"], mesh.shape["tp"])
    return jax.shard_map(
        functools.partial(body, sizes),
        mesh=mesh,
        in_specs=(
            P(("grp", "fs"), "tp"),
            P(),
            P("fs", "tp"),
            P("fs", "tp"),
            P("fs", "tp"),
            P(),
            P(None, "tp"),
            P("tp"),
            P(),
            P("tp", "fs"),
            P(),
            P("fs", "tp"),
            P("fs", "tp"),
            P("tp", "fs"),
            P("tp"),
        ),
        out_specs=P(("grp", "fs"), "tp"),
        check_vma=False,
    )
```

```python
import functools

import jax
import jax.numpy as jnp
from jax import lax
from jax.experimental import pallas as pl
from jax.experimental.pallas import tpu as pltpu
from jax.sharding import PartitionSpec as P

DK = 128
DV = 256
BLOCK = 64
epsilon = 1e-06
highest = lax.Precision.HIGHEST
MESH = pl.DeviceIdType.MESH
LANES = 128
HALVES = 2


def unit_chunks(units):
    if units % LANES:
        return [(0, units)]
    tiles = units // LANES
    pieces = [-(-tiles // 3) + (-(-tiles // 3)) % 2] * 3
    chunks, start = [], 0
    for piece in pieces:
        size = min(piece, tiles - start)
        if size > 0:
            chunks.append((start * LANES, size * LANES))
            start += size
    return chunks


def down_columns(columns):
    return 2 * LANES if columns % (2 * LANES) == 0 else LANES


def down_parts(columns):
    if columns % (2 * LANES):
        return [(0, columns)]
    parts = [(at, 2 * LANES) for at in range(0, columns, 2 * LANES)]
    at, size = parts.pop()
    return parts + [(at, LANES), (at + LANES, LANES)]


def layer_kernel(
    sizes,
    tokens_ref,
    attn_gain_ref,
    w_low_ref,
    w_lift_ref,
    decay_bias_ref,
    head_gain_ref,
    ffn_gain_ref,
    final_gain_ref,
    w_query_ref,
    w_key_ref,
    w_value_ref,
    w_out_ref,
    w_gate_ref,
    w_up_ref,
    w_down_ref,
    result_ref,
    g_mix,
    g_out,
    g_gate,
    g_up,
    g_down,
    rows_all,
    normed,
    mix_rows,
    log_decay,
    mixed,
    state,
    partial_out,
    sib_out,
    far_out,
    first_all,
    hidden,
    partial_down,
    sib_down,
    far_down,
    sum_out,
    sum_in,
    second,
    squares,
    z_send,
    z_recv,
    y_send,
    y_recv,
    e_send,
    e_recv,
    e_last,
    ag_send,
    ag_recv,
    rs_send,
    rs_recv,
    dd_send,
    dd_recv,
    dx_send,
    dx_recv,
    guest_send,
    guest_recv,
    back_send,
    back_recv,
    sq_send,
    sq_recv,
    local_sem,
):
    n, tp = sizes
    chips = tp // 2
    g, f, t = lax.axis_index("grp"), lax.axis_index("fs"), lax.axis_index("tp")
    chip, core = t // 2, lax.rem(t, 2)
    sibling = t + 1 - 2 * core
    rows, width = tokens_ref.shape
    features = width * tp
    f32, bf16 = jnp.float32, jnp.bfloat16
    inner = jnp.logical_and(f > 0, f < n - 1)
    outer = jnp.logical_not(inner)
    has_guest = jnp.logical_or(f == 1, f == n - 2)
    guests = jnp.where(has_guest, 1, 0)
    guest_plane = jnp.where(f == 1, 0, n - 1)
    host_plane = jnp.where(f == 0, 1, n - 2)
    near = jnp.where(2 * f < n, 0, 1)
    far = 1 - near

    messages = []
    column = 0
    for w, parts in ((w_query_ref, 1), (w_key_ref, 1), (w_value_ref, 2)):
        size = w.shape[1] // parts
        for part in range(parts):
            messages.append((w, g_mix, part * size, column, size))
            column += size
    qkv = range(len(messages))
    size = down_columns(w_out_ref.shape[1])
    for at in range(0, w_out_ref.shape[1], size):
        messages.append((w_out_ref, g_out, at, at, size))
    n_mix = len(messages)
    outs = range(len(qkv), n_mix)
    chunks = unit_chunks(w_gate_ref.shape[1])
    ffn_groups = []
    for start, size in chunks:
        ffn_groups.append((len(messages), len(messages) + 1))
        messages.append((w_gate_ref, g_gate, start, start, size))
        messages.append((w_up_ref, g_up, start, start, size))
    cols = w_down_ref.shape[1]
    split = down_parts(cols)
    pieces = len(split)
    down_at = len(messages)
    for start, size in split:
        messages.append((w_down_ref, g_down, start, start, size))
    down_groups = [(down_at + c,) for c in range(pieces)]
    total_messages = len(messages)
    last_down = total_messages - 1
    last_size = messages[last_down][4]
    holders = [g_mix, g_out, g_gate, g_up, g_down]
    groups = [tuple(qkv), tuple(outs)] + ffn_groups + down_groups
    group_of = {m: i for i, group in enumerate(groups) for m in group}

    def holder_of(m):
        return [i for i, held in enumerate(holders) if held is messages[m][1]][0]

    def is_ffn(m):
        return m >= n_mix

    def comes_whole(m, step):
        return step == 1 and (is_ffn(m) or m in qkv)

    def steps_of(m):
        return n - 2 if is_ffn(m) else n - 1

    barrier = pltpu.get_barrier_semaphore()

    @pl.when(f > 0)
    def _():
        pl.semaphore_signal(barrier, inc=1, device_id=(g, f - 1, t), device_id_type=MESH)

    @pl.when(f < n - 1)
    def _():
        pl.semaphore_signal(barrier, inc=1, device_id=(g, f + 1, t), device_id_type=MESH)

    pl.semaphore_signal(barrier, inc=1, device_id=(1 - g, f, t), device_id_type=MESH)
    for d in range(1, tp):
        peer = lax.rem(t + d, tp)
        pl.semaphore_signal(barrier, inc=1, device_id=(g, f, peer), device_id_type=MESH)
    met = jnp.where(f > 0, 1, 0) + jnp.where(f < n - 1, 1, 0) + tp
    pl.semaphore_wait(barrier, met)

    def half_of(w, which):
        part = w.shape[0] // 2
        return pl.ds(pl.multiple_of(which * part, 16), part)

    def toward(way):
        return f + 1 - 2 * way

    def ring_copy(source, at, send, recv, way):
        return pltpu.make_async_remote_copy(
            source, at, send, recv, device_id=(g, toward(way), t), device_id_type=MESH
        )

    def place(m, owner, which):
        w, held, start, column, columns = messages[m]
        return held.at[owner, half_of(w, which), pl.ds(column, columns)]

    def source_of(m, which):
        w, held, start, column, columns = messages[m]
        return w.at[half_of(w, which), pl.ds(start, columns)]

    def z_copy(m, way, step):
        owner = f + (step - 1) * (2 * way - 1)
        at = place(m, owner, g)
        source = source_of(m, g) if step == 1 else at
        return ring_copy(
            source, at, z_send.at[holder_of(m), owner + way], z_recv.at[m, owner], way
        )

    def received(m, way, step):
        owner = f + step * (2 * way - 1)
        at = place(m, owner, g)
        return ring_copy(at, at, z_send.at[holder_of(m), owner + way], z_recv.at[m, owner], way)

    def e_copy(m, way, owner):
        send = e_last.at[way] if m == last_down else e_send.at[holder_of(m)]
        at = place(m, owner, 1 - g)
        return ring_copy(source_of(m, 1 - g), at, send, e_recv.at[group_of[m], way], way)

    def y_copy(m, way, step):
        owner = f + step * (2 * way - 1)
        at = place(m, owner, g)
        return pltpu.make_async_remote_copy(
            at, at, y_send.at[holder_of(m), owner], y_recv.at[group_of[m], owner],
            device_id=(1 - g, f, t), device_id_type=MESH,
        )

    def bytes_of(i, owner):
        m = groups[i][0]
        w, held, start, column, columns = messages[m]
        if i < 2:
            return held.at[owner, half_of(w, g), :]
        if len(groups[i]) == 2:
            return held.at[owner, :, pl.ds(column, columns)]
        return place(m, owner, g)

    def whole_here(i, way):
        at = bytes_of(i, f + 2 * way - 1)
        return ring_copy(at, at, e_last.at[way], e_recv.at[i, way], way)

    def y_here(i, way, step):
        owner = f + step * (2 * way - 1)
        at = bytes_of(i, owner)
        return pltpu.make_async_remote_copy(
            at, at, y_send.at[0, owner], y_recv.at[i, owner],
            device_id=(1 - g, f, t), device_id_type=MESH,
        )

    def gets(m, way, step):
        j = f + step * (2 * way - 1)
        there = jnp.logical_and(j >= 0, j < n)
        return jnp.logical_and(there, inner) if is_ffn(m) else there

    def gives(m, way, step):
        j = f + (step - 1) * (2 * way - 1)
        there = jnp.logical_and(j >= 0, j < n)
        to = toward(way)
        low, high = (1, n - 2) if is_ffn(m) else (0, n - 1)
        return jnp.logical_and(there, jnp.logical_and(to >= low, to <= high))

    def gives_whole(m, way):
        if m == last_down:
            return gives(m, way, 1)
        return f == jnp.where(way == 0, 0, n - 1)

    def gets_whole(m, way):
        if m == last_down:
            return gets(m, way, 1)
        return f == jnp.where(way == 0, 1, n - 2)

    def launch(group, way):
        for m in group:
            @pl.when(gives(m, way, 1))
            def _():
                z_copy(m, way, 1).start()

    def complete(group):
        for way in (0, 1):
            for m in group:
                @pl.when(gives_whole(m, way))
                def _():
                    e_copy(m, way, f).start()

    def tick(group, way, step):
        for m in group:
            if step > steps_of(m):
                continue

            @pl.when(gets(m, way, step))
            def _():
                received(m, way, step).wait_recv()
                if comes_whole(m, step):
                    @pl.when(jnp.logical_not(gets_whole(m, way)))
                    def _():
                        y_copy(m, way, step).start()
                else:
                    y_copy(m, way, step).start()

            if step < steps_of(m):
                @pl.when(gives(m, way, step + 1))
                def _():
                    z_copy(m, way, step + 1).start()

    def arrived(i, way, step):
        m = groups[i][0]
        if comes_whole(m, step):
            whole = gets_whole(m, way)

            @pl.when(whole)
            def _():
                whole_here(i, way).wait_recv()

            @pl.when(jnp.logical_not(whole))
            def _():
                y_here(i, way, step).wait_recv()
        else:
            y_here(i, way, step).wait_recv()

    def all_arrived(i):
        m = groups[i][0]
        for step in range(1, steps_of(m) + 1):
            for way in (0, 1):
                @pl.when(gets(m, way, step))
                def _():
                    arrived(i, way, step)

    def peer_of(e):
        return 2 * lax.rem(chip + e, chips) + core

    def from_of(e):
        return 2 * lax.rem(chip - e + chips, chips) + core

    def tp_copy(source, target, send, recv, peer):
        return pltpu.make_async_remote_copy(
            source, target, send, recv, device_id=(g, f, peer), device_id_type=MESH
        )

    def ag_copy(kind, slot, source, target, peer):
        return tp_copy(source, target, ag_send.at[kind], ag_recv.at[kind, slot], peer)

    others = range(1, tp)
    beyond = range(1, chips)

    def gather_out(kind, source, at):
        for e in beyond:
            ag_copy(kind, e, source, at(t), peer_of(e)).start()
        ag_copy(kind, 0, source, at(t), sibling).start()

    def gather_forward(kind, at):
        for e in beyond:
            came = at(from_of(e))
            ag_copy(kind, e, came, came, peer_of(e)).wait_recv()
            ag_copy(kind, chips - 1 + e, came, came, sibling).start()

    def gather_wait(kind, at):
        ag_copy(kind, 0, at(sibling), at(sibling), sibling).wait_recv()
        for e in beyond:
            came = at(from_of(e) + 1 - 2 * core)
            ag_copy(kind, chips - 1 + e, came, came, sibling).wait_recv()

    def gather_drain(kind, every):
        ag_copy(kind, 0, every, every, sibling).wait_send()

    def rows_of(h):
        return pl.ds(h * (rows // HALVES), rows // HALVES)

    def token_at(p):
        return rows_all.at[p]

    def first_at(r, h):
        return lambda p: first_all.at[r, p, rows_of(h)]

    def ag_kind(r, h):
        return 1 + r * HALVES + h

    def square_copy(d):
        peer = lax.rem(t + d, tp)
        return tp_copy(squares.at[0], squares.at[d], sq_send, sq_recv, peer)

    ahead = ffn_groups + down_groups
    ways = {"near": (near, n // 2 - 1), "far": (far, n - 2)}
    launched, ticked = set(), set()

    def send_own(i):
        if i < len(ahead) and i not in launched:
            launched.add(i)
            for way in (0, 1):
                launch(ahead[i], way)

    def relay(i, which, step=None):
        if i >= len(ahead):
            return
        way, top = ways[which]
        for s in range(1, top + 1):
            if step in (None, s) and (i, which, s) not in ticked:
                ticked.add((i, which, s))
                tick(ahead[i], way, s)

    def relayed(i):
        send_own(i)
        relay(i, "near")
        relay(i, "far")

    first_down = len(ffn_groups)

    def pump(k):
        for act in plan.get(k, ()):
            act()

    down_index = [len(ffn_groups) + c for c in range(len(down_groups))]

    def down_near():
        for i in down_index[1:]:
            relay(i, "near")

    def down_early():
        for i in down_index[1:]:
            relay(i, "far", 1)

    def down_own():
        for i in down_index:
            send_own(i)

    plan = {
        -1: [lambda: send_own(0)],
        0: [lambda: relay(0, "near"), lambda: send_own(1)],
        1: [lambda: relay(0, "far", 1)],
        2: [lambda: relay(1, "near"), lambda: send_own(2), lambda: relay(0, "far")],
        4: [lambda: relay(1, "far", 1)],
        14: [lambda: relay(1, "far")],
        5: [lambda: relay(2, "near"), down_own],
        6: [lambda: relay(2, "far", 1)],
        12: [lambda: relay(2, "far")],
        7: [lambda: relay(3, "far", 1)],
        8: [lambda: relay(3, "near"), down_early],
        9: [down_near, lambda: complete(down_groups[-1])],
        10: [lambda: relay(3, "far")],
    }

    def last_step(way):
        return jnp.where(way == 0, f, n - 1 - f)

    def after(step, way, group):
        @pl.when(last_step(way) == step)
        def _():
            launch(group, way)

    for way in (0, 1):
        launch(qkv, way)
        after(0, way, outs)

    @pl.when(outer)
    def _():
        complete(qkv)
        for group in ffn_groups[:-1]:
            for way in (0, 1):
                launch(group, way)
        for group in ffn_groups[:-1]:
            complete(group)
        for way in (0, 1):
            launch(ffn_groups[-1], way)

    gather_out(0, tokens_ref, token_at)
    locals_ = [pltpu.make_async_copy(tokens_ref, rows_all.at[t], local_sem.at[0])]
    own = [messages[m] for m in range(n_mix)]
    for index, (w, held, start, column, columns) in enumerate(own):
        at = held.at[f, :, pl.ds(column, columns)]
        source = w.at[:, pl.ds(start, columns)]
        locals_.append(pltpu.make_async_copy(source, at, local_sem.at[1 + index]))
    inner_locals = []
    for index, (w, held) in enumerate(((w_gate_ref, g_gate), (w_up_ref, g_up), (w_down_ref, g_down))):
        inner_locals.append(pltpu.make_async_copy(w, held.at[f], local_sem.at[1 + n_mix + index]))
    for copy in locals_:
        copy.start()

    @pl.when(inner)
    def _():
        for copy in inner_locals:
            copy.start()

    for step in range(1, n):
        for m in qkv:
            for way in (0, 1):
                tick((m,), way, step)
        for way in (0, 1):
            after(step, way, outs)
        if step == 1:
            gather_forward(0, token_at)
    for step in range(1, n // 2):
        tick(outs, near, step)
    pl.when(inner)(lambda: pump(-1))

    @pl.when(inner)
    def _():
        for copy in inner_locals:
            copy.wait()

    for copy in locals_:
        copy.wait()
    gather_wait(0, token_at)

    def normalize(source, slot, gain_ref, at):
        total = jnp.zeros((at.size, 1), f32)
        for p in range(tp):
            values = source[p, at].astype(f32)
            total += jnp.sum(values * values, axis=1, keepdims=True)
        factor = lax.rsqrt(total / features + epsilon)
        for p in range(tp):
            part = pl.ds(p * width, width)
            scaled = source[p, at].astype(f32) * factor * gain_ref[:, part]
            normed[slot, at, part] = scaled.astype(bf16)

    def product(lhs, held, at, size):
        block = held[:, :, pl.ds(at, size)]
        block = block.reshape(block.shape[0] * block.shape[1], size)
        return jnp.dot(lhs, block, preferred_element_type=f32)

    for h in range(HALVES):
        normalize(rows_all, 0, attn_gain_ref, rows_of(h))
    low_rank = lax.dot_general(
        normed[0], w_low_ref[...], (((1,), (1,)), ((), ())), preferred_element_type=f32
    )
    lifted = jnp.dot(low_rank.astype(bf16), w_lift_ref[...], preferred_element_type=f32)
    log_decay[...] = jax.nn.log_sigmoid(lifted + decay_bias_ref[...]) / 16.0

    all_arrived(0)
    tick(outs, far, 1)
    mix_block = 2 * LANES if mix_rows.shape[1] % (2 * LANES) == 0 else LANES

    def mix_step(i, carry):
        at = pl.multiple_of(i * mix_block, LANES)
        mix_rows[:, pl.ds(at, mix_block)] = product(normed[0], g_mix, at, mix_block).astype(bf16)
        return carry

    lax.fori_loop(0, mix_rows.shape[1] // mix_block, mix_step, 0)
    for step in range(2, n - 1):
        tick(outs, far, step)

    pl.when(inner)(lambda: pump(0))
    heads = mix_rows.shape[1] // (2 * DK + DV)
    at_row = lax.broadcasted_iota(jnp.int32, (BLOCK, BLOCK), 0)
    at_col = lax.broadcasted_iota(jnp.int32, (BLOCK, BLOCK), 1)
    causal = at_row >= at_col
    lower = causal.astype(bf16)

    def dot(a, b, ca, cb):
        return lax.dot_general(
            a, b, (((ca,), (cb,)), ((), ())), precision=highest, preferred_element_type=f32
        )

    def short_dot(a, b, ca, cb):
        a, b = a.astype(bf16), b.astype(bf16)
        return lax.dot_general(a, b, (((ca,), (cb,)), ((), ())), preferred_element_type=f32)

    state[...] = jnp.zeros_like(state)

    def block_step(here):
        decays = log_decay[here, :]
        high = decays.astype(bf16)
        low = decays - high.astype(f32)
        sums = short_dot(lower, high, 1, 0) + short_dot(lower, low, 1, 0)
        for h in range(heads):
            query = mix_rows[here, pl.ds(h * DK, DK)].astype(f32) * DK ** (-0.5)
            key = mix_rows[here, pl.ds((heads + h) * DK, DK)].astype(f32)
            value = mix_rows[here, pl.ds(2 * heads * DK + h * DV, DV)]
            cum = sums[:, h * DK : (h + 1) * DK]
            last = cum[BLOCK - 1 :, :]
            query_dec = (query * jnp.exp(cum)).astype(bf16)
            key_dec = key * jnp.exp(-cum)
            scores = jnp.where(causal, short_dot(query_dec, key_dec, 1, 1), 0.0)
            held = state[h]
            out = short_dot(scores, value, 1, 0) + short_dot(query_dec, held, 1, 1)
            state[h] = jnp.exp(last) * held + short_dot(value, key * jnp.exp(last - cum), 0, 0)
            factor = lax.rsqrt(jnp.mean(out * out, axis=1, keepdims=True) + epsilon)
            mixed[here, pl.ds(h * DV, DV)] = (out * factor * head_gain_ref[...]).astype(bf16)

    def gla(start, stop):
        for block in range(start, stop):
            block_step(pl.ds(block * BLOCK, BLOCK))

    blocks = rows // BLOCK
    gla(0, blocks // 2)
    pl.when(inner)(lambda: pump(1))
    tick(outs, far, n - 1)
    gla(blocks // 2, blocks)
    all_arrived(1)

    def block_place(place, size):
        return place // width, pl.ds(pl.multiple_of(lax.rem(place, width), LANES), size)

    def rs_copy(h, slot, source, target, peer):
        return tp_copy(source, target, rs_send.at[h], rs_recv.at[h, slot], peer)

    def sib_copy(h, c):
        return rs_copy(
            h, c, partial_out.at[2 * c + 1 - core, rows_of(h)], sib_out.at[c, rows_of(h)], sibling
        )

    def far_copy(h, e):
        return rs_copy(
            h, chips - 1 + e, partial_out.at[peer_of(e), rows_of(h)],
            far_out.at[e - 1, rows_of(h)], peer_of(e),
        )

    out_cols = g_out.shape[2]
    for h in range(HALVES):
        def out_step(j, carry):
            p, part = block_place(j * out_cols, out_cols)
            terms = jnp.dot(mixed[rows_of(h), :], g_out[j], preferred_element_type=f32)
            partial_out[p, rows_of(h), part] = terms.astype(bf16)
            return carry

        lax.fori_loop(0, n, out_step, 0)
        for c in range(chips):
            sib_copy(h, c).start()
    for h in range(HALVES):
        for c in range(chips):
            sib_copy(h, c).wait_recv()
        for e in beyond:
            there = lax.rem(chip + e, chips)
            p = peer_of(e)
            pair = partial_out[p, rows_of(h)].astype(f32) + sib_out[there, rows_of(h)].astype(f32)
            partial_out[p, rows_of(h)] = pair.astype(bf16)
            far_copy(h, e).start()
    pl.when(inner)(lambda: pump(2))

    def guest_copy(h):
        at = rows_of(h)
        return pltpu.make_async_remote_copy(
            first_all.at[0, t, at], first_all.at[1, t, at], guest_send.at[h], guest_recv.at[h],
            device_id=(g, host_plane, t), device_id_type=MESH,
        )

    for h in range(HALVES):
        for e in beyond:
            far_copy(h, e).wait_recv()
        total = partial_out[t, rows_of(h)].astype(f32) + sib_out[chip, rows_of(h)].astype(f32)
        for e in beyond:
            total += far_out[e - 1, rows_of(h)].astype(f32)
        first_all[0, t, rows_of(h)] = (rows_all[t, rows_of(h)].astype(f32) + total).astype(bf16)

        @pl.when(inner)
        def _():
            gather_out(ag_kind(0, h), first_all.at[0, t, rows_of(h)], first_at(0, h))

        @pl.when(outer)
        def _():
            guest_copy(h).start()

    @pl.when(outer)
    def _():
        complete(ffn_groups[-1])
        for way in (0, 1):
            for group in down_groups:
                launch(group, way)
        for group in down_groups:
            complete(group)

    def units_step(r, start, size):
        gate = product(normed[r], g_gate, start, size)
        up = product(normed[r], g_up, start, size)
        hidden[r, :, pl.ds(start, size)] = (gate / (1.0 + jnp.exp(-gate)) * up).astype(bf16)

    def ffn_chunk(ci, r):
        start, size = chunks[ci]
        block = 2 * LANES
        whole = size // block

        def step(i, carry):
            units_step(r, pl.multiple_of(start + i * block, LANES), block)
            return carry

        lax.fori_loop(0, whole, step, 0)
        if size % block:
            units_step(r, start + whole * block, size % block)

    def guest_gather():
        for h in range(HALVES):
            guest_copy(h).wait_recv()
            gather_out(ag_kind(1, h), first_all.at[1, t, rows_of(h)], first_at(1, h))

    def guest_forward():
        for h in range(HALVES):
            gather_forward(ag_kind(1, h), first_at(1, h))

    def guest_ready():
        for h in range(HALVES):
            gather_wait(ag_kind(1, h), first_at(1, h))
            normalize(first_all.at[1], 1, ffn_gain_ref, rows_of(h))

    def place_of(j, c):
        p, part = block_place(j * cols + split[c][0], split[c][1])
        return p, part

    def dd_copy(r, j, c):
        p, part = place_of(j, c)
        return tp_copy(
            partial_down.at[r, p, :, part], sib_down.at[r, p // 2, :, part],
            dd_send.at[j * pieces + c, r], dd_recv.at[j * pieces + c, r], sibling,
        )

    def dx_copy(r, j, c, e):
        p, part = place_of(j, c)
        return tp_copy(
            partial_down.at[r, p, :, part], far_down.at[r, e - 1, :, part],
            dx_send.at[j * pieces + c, r, e - 1], dx_recv.at[j * pieces + c, r, e - 1],
            2 * (p // 2) + core,
        )

    def down_compute(j, c, r):
        p, part = place_of(j, c)
        terms = jnp.dot(hidden[r], g_down[j, :, pl.ds(*split[c])], preferred_element_type=f32)
        partial_down[r, p, :, part] = terms.astype(bf16)

        @pl.when(lax.rem(p, 2) != core)
        def _():
            dd_copy(r, j, c).start()

    def down_pass(j, c, r):
        p, part = place_of(j, c)

        @pl.when(jnp.logical_and(lax.rem(p, 2) == core, p // 2 != chip))
        def _():
            dd_copy(r, j, c).wait_recv()
            pair = partial_down[r, p, :, part].astype(f32)
            pair += sib_down[r, p // 2, :, part].astype(f32)
            partial_down[r, p, :, part] = pair.astype(bf16)
            for e in beyond:
                @pl.when(lax.rem(chip + e, chips) == p // 2)
                def _():
                    dx_copy(r, j, c, e).start()

    def each_set(low, act):
        def one(i, carry):
            act(guests - i)
            return carry

        lax.fori_loop(0, guests + 1 - low, one, 0)

    squares[0] = jnp.zeros((8, rows), f32)

    def settle(part, values):
        second[:, part] = values
        squares[0] += dot(jnp.ones((8, part.size), f32), values * values, 1, 1)

    def back_copy(j, c):
        part = place_of(j, c)[1]
        k = j * pieces + c
        return pltpu.make_async_remote_copy(
            sum_out.at[:, part], sum_in.at[:, part], back_send, back_recv.at[k],
            device_id=(g, guest_plane, t), device_id_type=MESH,
        )

    def down_total(j, c, r):
        p, part = place_of(j, c)

        @pl.when(p == t)
        def _():
            def whole_of(r):
                dd_copy(r, j, c).wait_recv()
                for e in beyond:
                    dx_copy(r, j, c, e).wait_recv()
                total = partial_down[r, t, :, part].astype(f32)
                total += sib_down[r, chip, :, part].astype(f32)
                for e in beyond:
                    total += far_down[r, e - 1, :, part].astype(f32)
                return total

            if r:
                sum_out[:, part] = whole_of(r).astype(bf16)
                back_copy(j, c).start()
            else:
                settle(part, first_all[0, t, :, part].astype(f32) + whole_of(r))

    def drain_sends(which):
        for i in which:
            m = [m for m in range(total_messages) if holder_of(m) == i][0]
            held, w = holders[i], messages[m][0]
            width_of = held.shape[2]
            direct = width_of - last_size if i == 4 else width_of
            for step in range(1, steps_of(m) + 1):
                for way in (0, 1):
                    owner = f + (step - 1) * (2 * way - 1)

                    @pl.when(gives(m, way, step))
                    def _():
                        at = held.at[owner, half_of(w, g), :]
                        ring_copy(at, at, z_send.at[i, owner + way], z_recv.at[m, owner], way).wait_send()

                    got = gets(m, way, step)
                    size = width_of
                    if comes_whole(m, step):
                        got = jnp.logical_and(got, f != jnp.where(way == 0, 1, n - 2))
                        size = direct
                    came = f + step * (2 * way - 1)
                    if size:
                        @pl.when(got)
                        def _():
                            at = held.at[came, half_of(w, g), pl.ds(0, size)]
                            ring_copy(at, at, y_send.at[i, came], z_recv.at[m, came], way).wait_send()

                    if comes_whole(m, step) and direct:
                        @pl.when(f == jnp.where(way == 0, 0, n - 1))
                        def _():
                            at = held.at[f, half_of(w, g), pl.ds(0, direct)]
                            ring_copy(at, at, e_send.at[i], e_recv.at[0, way], way).wait_send()

                    if i == 4 and step == 1:
                        @pl.when(gives(last_down, way, 1))
                        def _():
                            e_copy(last_down, way, f).wait_send()

    def drain_mixer():
        gather_drain(0, rows_all.at[pl.ds(0, tp - 1)])
        for h in range(HALVES):
            every = partial_out.at[pl.ds(0, tp - 1), rows_of(h)]
            rs_copy(h, 0, every, every, sibling).wait_send()

    def drain_rows(r):
        for h in range(HALVES):
            gather_drain(ag_kind(r, h), first_all.at[r, pl.ds(0, tp - 1), rows_of(h)])

    def drain_down(r):
        for j in range(n):
            for c in range(pieces):
                p = (j * cols + split[c][0]) // width

                @pl.when(p % 2 != core)
                def _():
                    dd_copy(r, j, c).wait_send()

                for e in beyond:
                    @pl.when(jnp.logical_and(p % 2 == core, lax.rem(chip + e, chips) == p // 2))
                    def _():
                        dx_copy(r, j, c, e).wait_send()

    @pl.when(inner)
    def _():
        pump(4)
        for h in range(HALVES):
            gather_forward(ag_kind(0, h), first_at(0, h))
        for h in range(HALVES):
            gather_wait(ag_kind(0, h), first_at(0, h))
            normalize(first_all.at[0], 0, ffn_gain_ref, rows_of(h))
        last = len(chunks) - 1
        relayed(0)
        all_arrived(2)
        pump(14)
        ffn_chunk(0, 0)
        pump(5)
        pump(6)
        pl.when(has_guest)(guest_gather)
        if last > 1:
            relayed(1)
            all_arrived(3)
            ffn_chunk(1, 0)
        pl.when(has_guest)(guest_forward)
        pump(12)
        pl.when(has_guest)(guest_ready)
        pl.when(has_guest)(lambda: ffn_chunk(0, 1))
        pump(7)
        if last > 1:
            pl.when(has_guest)(lambda: ffn_chunk(1, 1))
        pump(8)
        if last > 0:
            relayed(last)
            all_arrived(2 + last)
            ffn_chunk(last, 0)
        pump(9)
        for c in range(pieces):
            down_compute(f, c, 0)
        if last > 0:
            pl.when(has_guest)(lambda: ffn_chunk(last, 1))
        for i in range(len(ahead)):
            send_own(i)
        pump(10)
        for c in range(pieces):
            down_pass(f, c, 0)
            pl.when(has_guest)(lambda: down_compute(f, c, 1))
        done = [(True, f, c) for c in range(pieces)]
        waiting = [lambda: [down_pass(f, c, 1) for c in range(pieces)] and None]
        waiting = [functools.partial(pl.when(has_guest), waiting[0])]

        def entry(which, step, c):
            way = ways[which][0]
            m, j = down_at + c, f + step * (2 * way - 1)
            valid = gets(m, way, step)
            relay(first_down + c, which, step)
            if which == "near":
                relay(first_down + c + 1, "far")
            if (which, step, c) == order[-1]:
                drain_sends(range(4))
                drain_mixer()
                drain_rows(0)
                pl.when(has_guest)(lambda: drain_rows(1))

            @pl.when(valid)
            def _():
                arrived(group_of[m], way, step)
                each_set(0, lambda r: down_compute(j, c, r))

            if waiting:
                waiting.pop()()
            done.append((valid, j, c))
            send = lambda: pl.when(valid)(lambda: each_set(0, lambda r: down_pass(j, c, r)))
            waiting.append(send)

        final = n - 2
        order = [("far", step, c) for c in range(pieces - 1) for step in range(1, final)]
        for c in range(pieces):
            order += [("near", step, c) for step in range(1, ways["near"][1] + 1)]
            if c == pieces - 1:
                order += [("far", step, c) for step in range(1, final)]
            order += [("far", final, c)]
        for which, step, c in order:
            entry(which, step, c)
        waiting.pop()()
        for r in (1, 0):
            for valid, j, c in done:
                guard = jnp.logical_and(valid, has_guest) if r else valid
                pl.when(guard)(lambda: down_total(j, c, r))

    @pl.when(outer)
    def _():
        drain_sends(range(5))
        drain_mixer()
        for h in range(HALVES):
            guest_copy(h).wait_send()
        for j in range(n):
            for c in range(pieces):
                p, part = place_of(j, c)

                @pl.when(p == t)
                def _():
                    back_copy(j, c).wait_recv()
                    total = sum_in[:, part].astype(f32)
                    settle(part, first_all[0, t, :, part].astype(f32) + total)

    for d in others:
        square_copy(d).start()
    sent, heard = squares.at[pl.ds(0, tp - 1)], squares.at[pl.ds(1, tp - 1)]
    tp_copy(sent, heard, sq_send, sq_recv, sibling).wait_recv()
    whole = squares[0]
    for d in others:
        whole += squares[d]
    factor = lax.rsqrt(jnp.transpose(whole) / features + epsilon)[:, :1]
    result_ref[...] = (second[...] * factor * final_gain_ref[...]).astype(bf16)

    tp_copy(sent, heard, sq_send, sq_recv, sibling).wait_send()

    @pl.when(inner)
    def _():
        drain_sends((4,))
        drain_down(0)

    @pl.when(has_guest)
    def _():
        drain_down(1)
        pltpu.make_async_remote_copy(
            sum_out, sum_in, back_send, back_recv.at[0],
            device_id=(g, guest_plane, t), device_id_type=MESH,
        ).wait_send()


def body(
    sizes, tokens, attn_gain, w_query, w_key, w_value, w_low, w_lift, decay_bias, head_gain,
    w_out, ffn_gain, w_gate, w_up, w_down, final_gain,
):
    n, tp = sizes
    rows, width = tokens.shape
    bf16, f32 = jnp.bfloat16, jnp.float32
    units, keys, values = w_gate.shape[1], w_query.shape[1], w_value.shape[1]
    mix_width = 2 * keys + values
    chips = tp // 2
    vmem = pltpu.VMEM
    held = [vmem((n, w_query.shape[0], mix_width), bf16)]
    held += [vmem((n, *w.shape), bf16) for w in (w_out, w_gate, w_up, w_down)]
    pieces = len(down_parts(w_down.shape[1]))
    messages = 4 + w_out.shape[1] // down_columns(w_out.shape[1])
    messages += 2 * len(unit_chunks(units)) + pieces
    groups = 2 + len(unit_chunks(units)) + pieces
    dma = pltpu.SemaphoreType.DMA
    anywhere = pl.BlockSpec(memory_space=pl.ANY)
    inside = pl.BlockSpec(memory_space=pltpu.VMEM)
    return pl.pallas_call(
        functools.partial(layer_kernel, sizes),
        name="layer",
        out_shape=jax.ShapeDtypeStruct((rows, width), bf16),
        in_specs=[anywhere] + [inside] * 7 + [anywhere] * 7,
        out_specs=inside,
        scratch_shapes=held + [
            vmem((tp, rows, width), bf16),
            vmem((2, rows, width * tp), bf16),
            vmem((rows, mix_width), bf16),
            vmem((rows, keys), f32),
            vmem((rows, values), bf16),
            vmem((keys // DK, DV, DK), f32),
            vmem((tp, rows, width), bf16),
            vmem((chips, rows, width), bf16),
            vmem((chips - 1, rows, width), bf16),
            vmem((2, tp, rows, width), bf16),
            vmem((2, rows, units), bf16),
            vmem((2, tp, rows, width), bf16),
            vmem((2, chips, rows, width), bf16),
            vmem((2, chips - 1, rows, width), bf16),
            vmem((rows, width), bf16),
            vmem((rows, width), bf16),
            vmem((rows, width), f32),
            vmem((tp, 8, rows), f32),
            dma((5, n + 1)),
            dma((messages, n)),
            dma((5, n)),
            dma((groups, n)),
            dma((5,)),
            dma((groups, 2)),
            dma((2,)),
            dma((1 + 2 * HALVES,)),
            dma((1 + 2 * HALVES, tp - 1)),
            dma((HALVES,)),
            dma((HALVES, tp - 1)),
            dma((n * pieces, 2)),
            dma((n * pieces, 2)),
            dma((n * pieces, 2, chips - 1)),
            dma((n * pieces, 2, chips - 1)),
            dma((HALVES,)),
            dma((HALVES,)),
            dma,
            dma((n * pieces,)),
            dma,
            dma,
            dma((12,)),
        ],
        compiler_params=pltpu.CompilerParams(
            collective_id=0, has_side_effects=True, vmem_limit_bytes=63 * 1024 * 1024
        ),
    )(
        tokens, attn_gain[None], w_low.T, w_lift, decay_bias[None], head_gain[None],
        ffn_gain[None], final_gain[None], w_query, w_key, w_value, w_out, w_gate, w_up, w_down,
    )


def solution(mesh):
    sizes = (mesh.shape["fs"], mesh.shape["tp"])
    return jax.shard_map(
        functools.partial(body, sizes),
        mesh=mesh,
        in_specs=(
            P(("grp", "fs"), "tp"),
            P(),
            P("fs", "tp"),
            P("fs", "tp"),
            P("fs", "tp"),
            P(),
            P(None, "tp"),
            P("tp"),
            P(),
            P("tp", "fs"),
            P(),
            P("fs", "tp"),
            P("fs", "tp"),
            P("tp", "fs"),
            P("tp"),
        ),
        out_specs=P(("grp", "fs"), "tp"),
        check_vma=False,
    )
```

```python
import functools

import jax
import jax.numpy as jnp
from jax import lax
from jax.experimental import pallas as pl
from jax.experimental.pallas import tpu as pltpu
from jax.sharding import PartitionSpec as P

DK = 128
DV = 256
BLOCK = 64
epsilon = 1e-06
highest = lax.Precision.HIGHEST
MESH = pl.DeviceIdType.MESH
LANES = 128
HALVES = 2


def unit_chunks(units):
    if units % LANES:
        return [(0, units)]
    tiles = units // LANES
    pieces = [-(-tiles // 3) + (-(-tiles // 3)) % 2] * 3
    chunks, start = [], 0
    for piece in pieces:
        size = min(piece, tiles - start)
        if size > 0:
            chunks.append((start * LANES, size * LANES))
            start += size
    return chunks


def down_columns(columns):
    return 2 * LANES if columns % (2 * LANES) == 0 else LANES


def down_parts(columns):
    if columns % (2 * LANES):
        return [(0, columns)]
    parts = [(at, 2 * LANES) for at in range(0, columns, 2 * LANES)]
    at, size = parts.pop()
    return parts + [(at, LANES), (at + LANES, LANES)]


def layer_kernel(
    sizes,
    tokens_ref,
    attn_gain_ref,
    w_low_ref,
    w_lift_ref,
    decay_bias_ref,
    head_gain_ref,
    ffn_gain_ref,
    final_gain_ref,
    w_query_ref,
    w_key_ref,
    w_value_ref,
    w_out_ref,
    w_gate_ref,
    w_up_ref,
    w_down_ref,
    result_ref,
    g_mix,
    g_out,
    g_gate,
    g_up,
    g_down,
    rows_all,
    normed,
    mix_rows,
    log_decay,
    mixed,
    state,
    partial_out,
    sib_out,
    far_out,
    first_all,
    hidden,
    partial_down,
    sib_down,
    far_down,
    sum_out,
    sum_in,
    second,
    squares,
    z_send,
    z_recv,
    y_send,
    y_recv,
    e_send,
    e_recv,
    e_last,
    ag_send,
    ag_recv,
    rs_send,
    rs_recv,
    dd_send,
    dd_recv,
    dx_send,
    dx_recv,
    guest_send,
    guest_recv,
    back_send,
    back_recv,
    sq_send,
    sq_recv,
    local_sem,
):
    n, tp = sizes
    chips = tp // 2
    g, f, t = lax.axis_index("grp"), lax.axis_index("fs"), lax.axis_index("tp")
    chip, core = t // 2, lax.rem(t, 2)
    sibling = t + 1 - 2 * core
    rows, width = tokens_ref.shape
    features = width * tp
    f32, bf16 = jnp.float32, jnp.bfloat16
    inner = jnp.logical_and(f > 0, f < n - 1)
    outer = jnp.logical_not(inner)
    has_guest = jnp.logical_or(f == 1, f == n - 2)
    guests = jnp.where(has_guest, 1, 0)
    guest_plane = jnp.where(f == 1, 0, n - 1)
    host_plane = jnp.where(f == 0, 1, n - 2)
    near = jnp.where(2 * f < n, 0, 1)
    far = 1 - near

    messages = []
    column = 0
    for w, parts in ((w_query_ref, 1), (w_key_ref, 1), (w_value_ref, 2)):
        size = w.shape[1] // parts
        for part in range(parts):
            messages.append((w, g_mix, part * size, column, size))
            column += size
    qkv = range(len(messages))
    size = down_columns(w_out_ref.shape[1])
    for at in range(0, w_out_ref.shape[1], size):
        messages.append((w_out_ref, g_out, at, at, size))
    n_mix = len(messages)
    outs = range(len(qkv), n_mix)
    chunks = unit_chunks(w_gate_ref.shape[1])
    ffn_groups = []
    for start, size in chunks:
        ffn_groups.append((len(messages), len(messages) + 1))
        messages.append((w_gate_ref, g_gate, start, start, size))
        messages.append((w_up_ref, g_up, start, start, size))
    cols = w_down_ref.shape[1]
    split = down_parts(cols)
    pieces = len(split)
    down_at = len(messages)
    for start, size in split:
        messages.append((w_down_ref, g_down, start, start, size))
    down_groups = [(down_at + c,) for c in range(pieces)]
    total_messages = len(messages)
    last_down = total_messages - 1
    last_size = messages[last_down][4]
    holders = [g_mix, g_out, g_gate, g_up, g_down]
    groups = [tuple(qkv), tuple(outs)] + ffn_groups + down_groups
    group_of = {m: i for i, group in enumerate(groups) for m in group}

    def holder_of(m):
        return [i for i, held in enumerate(holders) if held is messages[m][1]][0]

    def is_ffn(m):
        return m >= n_mix

    def comes_whole(m, step):
        return step == 1 and (is_ffn(m) or m in qkv)

    def steps_of(m):
        return n - 2 if is_ffn(m) else n - 1

    barrier = pltpu.get_barrier_semaphore()

    @pl.when(f > 0)
    def _():
        pl.semaphore_signal(barrier, inc=1, device_id=(g, f - 1, t), device_id_type=MESH)

    @pl.when(f < n - 1)
    def _():
        pl.semaphore_signal(barrier, inc=1, device_id=(g, f + 1, t), device_id_type=MESH)

    pl.semaphore_signal(barrier, inc=1, device_id=(1 - g, f, t), device_id_type=MESH)
    for d in range(1, tp):
        peer = lax.rem(t + d, tp)
        pl.semaphore_signal(barrier, inc=1, device_id=(g, f, peer), device_id_type=MESH)
    met = jnp.where(f > 0, 1, 0) + jnp.where(f < n - 1, 1, 0) + tp
    pl.semaphore_wait(barrier, met)

    def half_of(w, which):
        part = w.shape[0] // 2
        return pl.ds(pl.multiple_of(which * part, 16), part)

    def toward(way):
        return f + 1 - 2 * way

    def ring_copy(source, at, send, recv, way):
        return pltpu.make_async_remote_copy(
            source, at, send, recv, device_id=(g, toward(way), t), device_id_type=MESH
        )

    def place(m, owner, which):
        w, held, start, column, columns = messages[m]
        return held.at[owner, half_of(w, which), pl.ds(column, columns)]

    def source_of(m, which):
        w, held, start, column, columns = messages[m]
        return w.at[half_of(w, which), pl.ds(start, columns)]

    def z_copy(m, way, step):
        owner = f + (step - 1) * (2 * way - 1)
        at = place(m, owner, g)
        source = source_of(m, g) if step == 1 else at
        return ring_copy(
            source, at, z_send.at[holder_of(m), owner + way], z_recv.at[m, owner], way
        )

    def received(m, way, step):
        owner = f + step * (2 * way - 1)
        at = place(m, owner, g)
        return ring_copy(at, at, z_send.at[holder_of(m), owner + way], z_recv.at[m, owner], way)

    def e_copy(m, way, owner):
        send = e_last.at[way] if m == last_down else e_send.at[holder_of(m)]
        at = place(m, owner, 1 - g)
        return ring_copy(source_of(m, 1 - g), at, send, e_recv.at[group_of[m], way], way)

    def y_copy(m, way, step):
        owner = f + step * (2 * way - 1)
        at = place(m, owner, g)
        return pltpu.make_async_remote_copy(
            at, at, y_send.at[holder_of(m), owner], y_recv.at[group_of[m], owner],
            device_id=(1 - g, f, t), device_id_type=MESH,
        )

    def bytes_of(i, owner):
        m = groups[i][0]
        w, held, start, column, columns = messages[m]
        if i < 2:
            return held.at[owner, half_of(w, g), :]
        if len(groups[i]) == 2:
            return held.at[owner, :, pl.ds(column, columns)]
        return place(m, owner, g)

    def whole_here(i, way):
        at = bytes_of(i, f + 2 * way - 1)
        return ring_copy(at, at, e_last.at[way], e_recv.at[i, way], way)

    def y_here(i, way, step):
        owner = f + step * (2 * way - 1)
        at = bytes_of(i, owner)
        return pltpu.make_async_remote_copy(
            at, at, y_send.at[0, owner], y_recv.at[i, owner],
            device_id=(1 - g, f, t), device_id_type=MESH,
        )

    def gets(m, way, step):
        j = f + step * (2 * way - 1)
        there = jnp.logical_and(j >= 0, j < n)
        return jnp.logical_and(there, inner) if is_ffn(m) else there

    def gives(m, way, step):
        j = f + (step - 1) * (2 * way - 1)
        there = jnp.logical_and(j >= 0, j < n)
        to = toward(way)
        low, high = (1, n - 2) if is_ffn(m) else (0, n - 1)
        return jnp.logical_and(there, jnp.logical_and(to >= low, to <= high))

    def gives_whole(m, way):
        if m == last_down:
            return gives(m, way, 1)
        return f == jnp.where(way == 0, 0, n - 1)

    def gets_whole(m, way):
        if m == last_down:
            return gets(m, way, 1)
        return f == jnp.where(way == 0, 1, n - 2)

    def launch(group, way):
        for m in group:
            @pl.when(gives(m, way, 1))
            def _():
                z_copy(m, way, 1).start()

    def complete(group):
        for way in (0, 1):
            for m in group:
                @pl.when(gives_whole(m, way))
                def _():
                    e_copy(m, way, f).start()

    def tick(group, way, step):
        for m in group:
            if step > steps_of(m):
                continue

            @pl.when(gets(m, way, step))
            def _():
                received(m, way, step).wait_recv()
                if comes_whole(m, step):
                    @pl.when(jnp.logical_not(gets_whole(m, way)))
                    def _():
                        y_copy(m, way, step).start()
                else:
                    y_copy(m, way, step).start()

            if step < steps_of(m):
                @pl.when(gives(m, way, step + 1))
                def _():
                    z_copy(m, way, step + 1).start()

    def arrived(i, way, step):
        m = groups[i][0]
        if comes_whole(m, step):
            whole = gets_whole(m, way)

            @pl.when(whole)
            def _():
                whole_here(i, way).wait_recv()

            @pl.when(jnp.logical_not(whole))
            def _():
                y_here(i, way, step).wait_recv()
        else:
            y_here(i, way, step).wait_recv()

    def all_arrived(i):
        m = groups[i][0]
        for step in range(1, steps_of(m) + 1):
            for way in (0, 1):
                @pl.when(gets(m, way, step))
                def _():
                    arrived(i, way, step)

    def peer_of(e):
        return 2 * lax.rem(chip + e, chips) + core

    def from_of(e):
        return 2 * lax.rem(chip - e + chips, chips) + core

    def tp_copy(source, target, send, recv, peer):
        return pltpu.make_async_remote_copy(
            source, target, send, recv, device_id=(g, f, peer), device_id_type=MESH
        )

    def ag_copy(kind, slot, source, target, peer):
        return tp_copy(source, target, ag_send.at[kind], ag_recv.at[kind, slot], peer)

    others = range(1, tp)
    beyond = range(1, chips)

    def gather_out(kind, source, at):
        for e in beyond:
            ag_copy(kind, e, source, at(t), peer_of(e)).start()
        ag_copy(kind, 0, source, at(t), sibling).start()

    def gather_forward(kind, at):
        for e in beyond:
            came = at(from_of(e))
            ag_copy(kind, e, came, came, peer_of(e)).wait_recv()
            ag_copy(kind, chips - 1 + e, came, came, sibling).start()

    def gather_wait(kind, at):
        ag_copy(kind, 0, at(sibling), at(sibling), sibling).wait_recv()
        for e in beyond:
            came = at(from_of(e) + 1 - 2 * core)
            ag_copy(kind, chips - 1 + e, came, came, sibling).wait_recv()

    def gather_drain(kind, every):
        ag_copy(kind, 0, every, every, sibling).wait_send()

    def rows_of(h):
        return pl.ds(h * (rows // HALVES), rows // HALVES)

    def token_at(p):
        return rows_all.at[p]

    def first_at(r, h):
        return lambda p: first_all.at[r, p, rows_of(h)]

    def ag_kind(r, h):
        return 1 + r * HALVES + h

    def square_copy(d):
        peer = lax.rem(t + d, tp)
        return tp_copy(squares.at[0], squares.at[d], sq_send, sq_recv, peer)

    ahead = ffn_groups + down_groups
    ways = {"near": (near, n // 2 - 1), "far": (far, n - 2)}
    launched, ticked = set(), set()

    def send_own(i):
        if i < len(ahead) and i not in launched:
            launched.add(i)
            for way in (0, 1):
                launch(ahead[i], way)

    def relay(i, which, step=None):
        if i >= len(ahead):
            return
        way, top = ways[which]
        for s in range(1, top + 1):
            if step in (None, s) and (i, which, s) not in ticked:
                ticked.add((i, which, s))
                tick(ahead[i], way, s)

    def relayed(i):
        send_own(i)
        relay(i, "near")
        relay(i, "far")

    first_down = len(ffn_groups)

    def pump(k):
        for act in plan.get(k, ()):
            act()

    down_index = [len(ffn_groups) + c for c in range(len(down_groups))]

    def down_near():
        for i in down_index[1:]:
            relay(i, "near")

    def down_early():
        for i in down_index[1:]:
            relay(i, "far", 1)

    def down_own():
        for i in down_index:
            send_own(i)

    plan = {
        -1: [lambda: send_own(0)],
        0: [lambda: relay(0, "near"), lambda: send_own(1)],
        1: [lambda: relay(0, "far", 1)],
        2: [lambda: relay(1, "near"), lambda: send_own(2), lambda: relay(0, "far")],
        4: [lambda: relay(1, "far", 1)],
        14: [lambda: relay(1, "far")],
        5: [lambda: relay(2, "near"), down_own],
        6: [lambda: relay(2, "far", 1)],
        12: [lambda: relay(2, "far")],
        7: [lambda: relay(3, "far", 1)],
        8: [lambda: relay(3, "near"), down_early],
        9: [down_near, lambda: complete(down_groups[-1])],
        10: [lambda: relay(3, "far")],
    }

    def last_step(way):
        return jnp.where(way == 0, f, n - 1 - f)

    def after(step, way, group):
        @pl.when(last_step(way) == step)
        def _():
            launch(group, way)

    for way in (0, 1):
        launch(qkv, way)
        after(0, way, outs)

    @pl.when(outer)
    def _():
        complete(qkv)
        for group in ffn_groups[:-1]:
            for way in (0, 1):
                launch(group, way)
        for group in ffn_groups[:-1]:
            complete(group)
        for way in (0, 1):
            launch(ffn_groups[-1], way)

    gather_out(0, tokens_ref, token_at)
    locals_ = [pltpu.make_async_copy(tokens_ref, rows_all.at[t], local_sem.at[0])]
    own = [messages[m] for m in range(n_mix)]
    for index, (w, held, start, column, columns) in enumerate(own):
        at = held.at[f, :, pl.ds(column, columns)]
        source = w.at[:, pl.ds(start, columns)]
        locals_.append(pltpu.make_async_copy(source, at, local_sem.at[1 + index]))
    inner_locals = []
    for index, (w, held) in enumerate(((w_gate_ref, g_gate), (w_up_ref, g_up), (w_down_ref, g_down))):
        inner_locals.append(pltpu.make_async_copy(w, held.at[f], local_sem.at[1 + n_mix + index]))
    for copy in locals_:
        copy.start()

    @pl.when(inner)
    def _():
        for copy in inner_locals:
            copy.start()

    for step in range(1, n):
        for m in qkv:
            for way in (0, 1):
                tick((m,), way, step)
        for way in (0, 1):
            after(step, way, outs)
        if step == 1:
            gather_forward(0, token_at)
    for step in range(1, n // 2):
        tick(outs, near, step)
    pl.when(inner)(lambda: pump(-1))

    @pl.when(inner)
    def _():
        for copy in inner_locals:
            copy.wait()

    for copy in locals_:
        copy.wait()
    gather_wait(0, token_at)

    def normalize(source, slot, gain_ref, at):
        total = jnp.zeros((at.size, 1), f32)
        for p in range(tp):
            values = source[p, at].astype(f32)
            total += jnp.sum(values * values, axis=1, keepdims=True)
        factor = lax.rsqrt(total / features + epsilon)
        for p in range(tp):
            part = pl.ds(p * width, width)
            scaled = source[p, at].astype(f32) * factor * gain_ref[:, part]
            normed[slot, at, part] = scaled.astype(bf16)

    def product(lhs, held, at, size):
        block = held[:, :, pl.ds(at, size)]
        block = block.reshape(block.shape[0] * block.shape[1], size)
        return jnp.dot(lhs, block, preferred_element_type=f32)

    for h in range(HALVES):
        normalize(rows_all, 0, attn_gain_ref, rows_of(h))
    low_rank = lax.dot_general(
        normed[0], w_low_ref[...], (((1,), (1,)), ((), ())), preferred_element_type=f32
    )
    lifted = jnp.dot(low_rank.astype(bf16), w_lift_ref[...], preferred_element_type=f32)
    log_decay[...] = jax.nn.log_sigmoid(lifted + decay_bias_ref[...]) / 16.0

    all_arrived(0)
    tick(outs, far, 1)
    mix_block = 2 * LANES if mix_rows.shape[1] % (2 * LANES) == 0 else LANES

    def mix_step(i, carry):
        at = pl.multiple_of(i * mix_block, LANES)
        mix_rows[:, pl.ds(at, mix_block)] = product(normed[0], g_mix, at, mix_block).astype(bf16)
        return carry

    lax.fori_loop(0, mix_rows.shape[1] // mix_block, mix_step, 0)
    for step in range(2, n - 1):
        tick(outs, far, step)

    pl.when(inner)(lambda: pump(0))
    heads = mix_rows.shape[1] // (2 * DK + DV)
    at_row = lax.broadcasted_iota(jnp.int32, (BLOCK, BLOCK), 0)
    at_col = lax.broadcasted_iota(jnp.int32, (BLOCK, BLOCK), 1)
    causal = at_row >= at_col
    lower = causal.astype(bf16)

    def dot(a, b, ca, cb):
        return lax.dot_general(
            a, b, (((ca,), (cb,)), ((), ())), precision=highest, preferred_element_type=f32
        )

    def short_dot(a, b, ca, cb):
        a, b = a.astype(bf16), b.astype(bf16)
        return lax.dot_general(a, b, (((ca,), (cb,)), ((), ())), preferred_element_type=f32)

    state[...] = jnp.zeros_like(state)

    def block_step(here):
        decays = log_decay[here, :]
        high = decays.astype(bf16)
        low = decays - high.astype(f32)
        sums = short_dot(lower, high, 1, 0) + short_dot(lower, low, 1, 0)
        for h in range(heads):
            query = mix_rows[here, pl.ds(h * DK, DK)].astype(f32) * DK ** (-0.5)
            key = mix_rows[here, pl.ds((heads + h) * DK, DK)].astype(f32)
            value = mix_rows[here, pl.ds(2 * heads * DK + h * DV, DV)]
            cum = sums[:, h * DK : (h + 1) * DK]
            last = cum[BLOCK - 1 :, :]
            query_dec = (query * jnp.exp(cum)).astype(bf16)
            key_dec = key * jnp.exp(-cum)
            scores = jnp.where(causal, short_dot(query_dec, key_dec, 1, 1), 0.0)
            held = state[h]
            out = short_dot(scores, value, 1, 0) + short_dot(query_dec, held, 1, 1)
            state[h] = jnp.exp(last) * held + short_dot(value, key * jnp.exp(last - cum), 0, 0)
            factor = lax.rsqrt(jnp.mean(out * out, axis=1, keepdims=True) + epsilon)
            mixed[here, pl.ds(h * DV, DV)] = (out * factor * head_gain_ref[...]).astype(bf16)

    def gla(start, stop):
        for block in range(start, stop):
            block_step(pl.ds(block * BLOCK, BLOCK))

    blocks = rows // BLOCK
    gla(0, blocks // 2)
    pl.when(inner)(lambda: pump(1))
    tick(outs, far, n - 1)
    gla(blocks // 2, blocks)
    all_arrived(1)

    def block_place(place, size):
        return place // width, pl.ds(pl.multiple_of(lax.rem(place, width), LANES), size)

    def rs_copy(h, slot, source, target, peer):
        return tp_copy(source, target, rs_send.at[h], rs_recv.at[h, slot], peer)

    def sib_copy(h, c):
        return rs_copy(
            h, c, partial_out.at[2 * c + 1 - core, rows_of(h)], sib_out.at[c, rows_of(h)], sibling
        )

    def far_copy(h, e):
        return rs_copy(
            h, chips - 1 + e, partial_out.at[peer_of(e), rows_of(h)],
            far_out.at[e - 1, rows_of(h)], peer_of(e),
        )

    out_cols = g_out.shape[2]
    for h in range(HALVES):
        def out_step(j, carry):
            p, part = block_place(j * out_cols, out_cols)
            terms = jnp.dot(mixed[rows_of(h), :], g_out[j], preferred_element_type=f32)
            partial_out[p, rows_of(h), part] = terms.astype(bf16)
            return carry

        lax.fori_loop(0, n, out_step, 0)
        for c in range(chips):
            sib_copy(h, c).start()
    for h in range(HALVES):
        for c in range(chips):
            sib_copy(h, c).wait_recv()
        for e in beyond:
            there = lax.rem(chip + e, chips)
            p = peer_of(e)
            pair = partial_out[p, rows_of(h)].astype(f32) + sib_out[there, rows_of(h)].astype(f32)
            partial_out[p, rows_of(h)] = pair.astype(bf16)
            far_copy(h, e).start()
    pl.when(inner)(lambda: pump(2))

    def guest_copy(h):
        at = rows_of(h)
        return pltpu.make_async_remote_copy(
            first_all.at[0, t, at], first_all.at[1, t, at], guest_send.at[h], guest_recv.at[h],
            device_id=(g, host_plane, t), device_id_type=MESH,
        )

    for h in range(HALVES):
        for e in beyond:
            far_copy(h, e).wait_recv()
        total = partial_out[t, rows_of(h)].astype(f32) + sib_out[chip, rows_of(h)].astype(f32)
        for e in beyond:
            total += far_out[e - 1, rows_of(h)].astype(f32)
        first_all[0, t, rows_of(h)] = (rows_all[t, rows_of(h)].astype(f32) + total).astype(bf16)

        @pl.when(inner)
        def _():
            gather_out(ag_kind(0, h), first_all.at[0, t, rows_of(h)], first_at(0, h))

        @pl.when(outer)
        def _():
            guest_copy(h).start()

    @pl.when(outer)
    def _():
        complete(ffn_groups[-1])
        for way in (0, 1):
            for group in down_groups:
                launch(group, way)
        for group in down_groups:
            complete(group)

    def units_step(r, start, size):
        gate = product(normed[r], g_gate, start, size)
        up = product(normed[r], g_up, start, size)
        hidden[r, :, pl.ds(start, size)] = (gate / (1.0 + jnp.exp(-gate)) * up).astype(bf16)

    def ffn_chunk(ci, r):
        start, size = chunks[ci]
        block = 2 * LANES
        whole = size // block

        def step(i, carry):
            units_step(r, pl.multiple_of(start + i * block, LANES), block)
            return carry

        lax.fori_loop(0, whole, step, 0)
        if size % block:
            units_step(r, start + whole * block, size % block)

    def guest_gather():
        for h in range(HALVES):
            guest_copy(h).wait_recv()
            gather_out(ag_kind(1, h), first_all.at[1, t, rows_of(h)], first_at(1, h))

    def guest_forward():
        for h in range(HALVES):
            gather_forward(ag_kind(1, h), first_at(1, h))

    def guest_ready():
        for h in range(HALVES):
            gather_wait(ag_kind(1, h), first_at(1, h))
            normalize(first_all.at[1], 1, ffn_gain_ref, rows_of(h))

    def place_of(j, c):
        p, part = block_place(j * cols + split[c][0], split[c][1])
        return p, part

    per = max(1, width // cols)

    def slot_of(j, c):
        return lax.rem(j, per) * pieces + c

    def dd_copy(r, j, c):
        p, part = place_of(j, c)
        return tp_copy(
            partial_down.at[r, p, :, part], sib_down.at[r, p // 2, :, part],
            dd_send.at[r], dd_recv.at[j * pieces + c, r], sibling,
        )

    def dx_copy(r, j, c, e):
        p, part = place_of(j, c)
        return tp_copy(
            partial_down.at[r, p, :, part], far_down.at[r, e - 1, :, part],
            dx_send.at[r], dx_recv.at[slot_of(j, c), r, e - 1],
            2 * (p // 2) + core,
        )

    def down_compute(j, c, r):
        p, part = place_of(j, c)
        terms = jnp.dot(hidden[r], g_down[j, :, pl.ds(*split[c])], preferred_element_type=f32)
        partial_down[r, p, :, part] = terms.astype(bf16)

        @pl.when(lax.rem(p, 2) != core)
        def _():
            dd_copy(r, j, c).start()

    def down_pass(j, c, r):
        p, part = place_of(j, c)

        @pl.when(jnp.logical_and(lax.rem(p, 2) == core, p // 2 != chip))
        def _():
            dd_copy(r, j, c).wait_recv()
            pair = partial_down[r, p, :, part].astype(f32)
            pair += sib_down[r, p // 2, :, part].astype(f32)
            partial_down[r, p, :, part] = pair.astype(bf16)
            for e in beyond:
                @pl.when(lax.rem(chip + e, chips) == p // 2)
                def _():
                    dx_copy(r, j, c, e).start()

    def each_set(low, act):
        def one(i, carry):
            act(guests - i)
            return carry

        lax.fori_loop(0, guests + 1 - low, one, 0)

    squares[0] = jnp.zeros((8, rows), f32)

    def settle(part, values):
        second[:, part] = values
        squares[0] += dot(jnp.ones((8, part.size), f32), values * values, 1, 1)

    def back_copy(j, c):
        part = place_of(j, c)[1]
        k = slot_of(j, c)
        return pltpu.make_async_remote_copy(
            sum_out.at[:, part], sum_in.at[:, part], back_send, back_recv.at[k],
            device_id=(g, guest_plane, t), device_id_type=MESH,
        )

    def down_total(j, c, r):
        p, part = place_of(j, c)

        @pl.when(p == t)
        def _():
            def whole_of(r):
                dd_copy(r, j, c).wait_recv()
                for e in beyond:
                    dx_copy(r, j, c, e).wait_recv()
                total = partial_down[r, t, :, part].astype(f32)
                total += sib_down[r, chip, :, part].astype(f32)
                for e in beyond:
                    total += far_down[r, e - 1, :, part].astype(f32)
                return total

            if r:
                sum_out[:, part] = whole_of(r).astype(bf16)
                back_copy(j, c).start()
            else:
                settle(part, first_all[0, t, :, part].astype(f32) + whole_of(r))

    def drain_sends(which):
        for i in which:
            m = [m for m in range(total_messages) if holder_of(m) == i][0]
            held, w = holders[i], messages[m][0]
            width_of = held.shape[2]
            direct = width_of - last_size if i == 4 else width_of
            for step in range(1, steps_of(m) + 1):
                for way in (0, 1):
                    owner = f + (step - 1) * (2 * way - 1)

                    @pl.when(gives(m, way, step))
                    def _():
                        at = held.at[owner, half_of(w, g), :]
                        ring_copy(at, at, z_send.at[i, owner + way], z_recv.at[m, owner], way).wait_send()

                    got = gets(m, way, step)
                    size = width_of
                    if comes_whole(m, step):
                        got = jnp.logical_and(got, f != jnp.where(way == 0, 1, n - 2))
                        size = direct
                    came = f + step * (2 * way - 1)
                    if size:
                        @pl.when(got)
                        def _():
                            at = held.at[came, half_of(w, g), pl.ds(0, size)]
                            ring_copy(at, at, y_send.at[i, came], z_recv.at[m, came], way).wait_send()

                    if comes_whole(m, step) and direct:
                        @pl.when(f == jnp.where(way == 0, 0, n - 1))
                        def _():
                            at = held.at[f, half_of(w, g), pl.ds(0, direct)]
                            ring_copy(at, at, e_send.at[i], e_recv.at[0, way], way).wait_send()

                    if i == 4 and step == 1:
                        @pl.when(gives(last_down, way, 1))
                        def _():
                            e_copy(last_down, way, f).wait_send()

    def drain_mixer():
        gather_drain(0, rows_all.at[pl.ds(0, tp - 1)])
        for h in range(HALVES):
            every = partial_out.at[pl.ds(0, tp - 1), rows_of(h)]
            rs_copy(h, 0, every, every, sibling).wait_send()

    def drain_rows(r):
        for h in range(HALVES):
            gather_drain(ag_kind(r, h), first_all.at[r, pl.ds(0, tp - 1), rows_of(h)])

    def drain_down(r):
        every = partial_down.at[r, pl.ds(0, chips)]
        tp_copy(every, every, dd_send.at[r], dd_recv.at[0, r], sibling).wait_send()
        if chips > 1:
            every = partial_down.at[r, pl.ds(0, chips - 1)]
            tp_copy(every, every, dx_send.at[r], dd_recv.at[0, r], sibling).wait_send()

    @pl.when(inner)
    def _():
        pump(4)
        for h in range(HALVES):
            gather_forward(ag_kind(0, h), first_at(0, h))
        for h in range(HALVES):
            gather_wait(ag_kind(0, h), first_at(0, h))
            normalize(first_all.at[0], 0, ffn_gain_ref, rows_of(h))
        last = len(chunks) - 1
        relayed(0)
        all_arrived(2)
        pump(14)
        ffn_chunk(0, 0)
        pump(5)
        pump(6)
        pl.when(has_guest)(guest_gather)
        if last > 1:
            relayed(1)
            all_arrived(3)
            ffn_chunk(1, 0)
        pl.when(has_guest)(guest_forward)
        pump(12)
        pl.when(has_guest)(guest_ready)
        pl.when(has_guest)(lambda: ffn_chunk(0, 1))
        pump(7)
        if last > 1:
            pl.when(has_guest)(lambda: ffn_chunk(1, 1))
        pump(8)
        if last > 0:
            relayed(last)
            all_arrived(2 + last)
            ffn_chunk(last, 0)
        pump(9)
        for c in range(pieces):
            down_compute(f, c, 0)
        if last > 0:
            pl.when(has_guest)(lambda: ffn_chunk(last, 1))
        for i in range(len(ahead)):
            send_own(i)
        pump(10)
        for c in range(pieces):
            down_pass(f, c, 0)
            pl.when(has_guest)(lambda: down_compute(f, c, 1))
        done = [(True, f, c) for c in range(pieces)]
        waiting = [lambda: [down_pass(f, c, 1) for c in range(pieces)] and None]
        waiting = [functools.partial(pl.when(has_guest), waiting[0])]

        def entry(which, step, c):
            way = ways[which][0]
            m, j = down_at + c, f + step * (2 * way - 1)
            valid = gets(m, way, step)
            relay(first_down + c, which, step)
            if which == "near":
                relay(first_down + c + 1, "far")
            if (which, step, c) == ("far", final, 0):
                drain_sends(range(4))
                drain_mixer()
                drain_rows(0)
                pl.when(has_guest)(lambda: drain_rows(1))

            @pl.when(valid)
            def _():
                arrived(group_of[m], way, step)
                each_set(0, lambda r: down_compute(j, c, r))

            if waiting:
                waiting.pop()()
            done.append((valid, j, c))
            if order.index((which, step, c)) < order.index(("far", final, 0)):
                send = lambda: pl.when(valid)(lambda: each_set(0, lambda r: down_pass(j, c, r)))
            else:
                guest = jnp.logical_and(valid, has_guest)
                send = lambda: pl.when(guest)(lambda: down_pass(j, c, 1))
                owed.append(lambda: pl.when(valid)(lambda: down_pass(j, c, 0)))
            waiting.append(send)

        final = n - 2
        order = [("far", step, c) for c in range(pieces - 1) for step in range(1, final)]
        for c in range(pieces):
            order += [("near", step, c) for step in range(1, ways["near"][1] + 1)]
            if c == pieces - 1:
                order += [("far", step, c) for step in range(1, final)]
            order += [("far", final, c)]
        owed = []
        for which, step, c in order:
            entry(which, step, c)
        waiting.pop()()
        for send in owed:
            send()
        for r in (1, 0):
            for valid, j, c in done:
                guard = jnp.logical_and(valid, has_guest) if r else valid
                pl.when(guard)(lambda: down_total(j, c, r))

    @pl.when(outer)
    def _():
        drain_sends(range(5))
        drain_mixer()
        for h in range(HALVES):
            guest_copy(h).wait_send()
        for j in range(n):
            for c in range(pieces):
                p, part = place_of(j, c)

                @pl.when(p == t)
                def _():
                    back_copy(j, c).wait_recv()
                    total = sum_in[:, part].astype(f32)
                    settle(part, first_all[0, t, :, part].astype(f32) + total)

    for d in others:
        square_copy(d).start()
    sent, heard = squares.at[pl.ds(0, tp - 1)], squares.at[pl.ds(1, tp - 1)]
    tp_copy(sent, heard, sq_send, sq_recv, sibling).wait_recv()
    whole = squares[0]
    for d in others:
        whole += squares[d]
    factor = lax.rsqrt(jnp.transpose(whole) / features + epsilon)[:, :1]
    result_ref[...] = (second[...] * factor * final_gain_ref[...]).astype(bf16)

    tp_copy(sent, heard, sq_send, sq_recv, sibling).wait_send()

    @pl.when(inner)
    def _():
        drain_sends((4,))
        drain_down(0)

    @pl.when(has_guest)
    def _():
        drain_down(1)
        pltpu.make_async_remote_copy(
            sum_out, sum_in, back_send, back_recv.at[0],
            device_id=(g, guest_plane, t), device_id_type=MESH,
        ).wait_send()


def body(
    sizes, tokens, attn_gain, w_query, w_key, w_value, w_low, w_lift, decay_bias, head_gain,
    w_out, ffn_gain, w_gate, w_up, w_down, final_gain,
):
    n, tp = sizes
    rows, width = tokens.shape
    bf16, f32 = jnp.bfloat16, jnp.float32
    units, keys, values = w_gate.shape[1], w_query.shape[1], w_value.shape[1]
    mix_width = 2 * keys + values
    chips = tp // 2
    vmem = pltpu.VMEM
    held = [vmem((n, w_query.shape[0], mix_width), bf16)]
    held += [vmem((n, *w.shape), bf16) for w in (w_out, w_gate, w_up, w_down)]
    pieces = len(down_parts(w_down.shape[1]))
    per = max(1, width // w_down.shape[1])
    messages = 4 + w_out.shape[1] // down_columns(w_out.shape[1])
    messages += 2 * len(unit_chunks(units)) + pieces
    groups = 2 + len(unit_chunks(units)) + pieces
    dma = pltpu.SemaphoreType.DMA
    anywhere = pl.BlockSpec(memory_space=pl.ANY)
    inside = pl.BlockSpec(memory_space=pltpu.VMEM)
    return pl.pallas_call(
        functools.partial(layer_kernel, sizes),
        name="layer",
        out_shape=jax.ShapeDtypeStruct((rows, width), bf16),
        in_specs=[anywhere] + [inside] * 7 + [anywhere] * 7,
        out_specs=inside,
        scratch_shapes=held + [
            vmem((tp, rows, width), bf16),
            vmem((2, rows, width * tp), bf16),
            vmem((rows, mix_width), bf16),
            vmem((rows, keys), f32),
            vmem((rows, values), bf16),
            vmem((keys // DK, DV, DK), f32),
            vmem((tp, rows, width), bf16),
            vmem((chips, rows, width), bf16),
            vmem((chips - 1, rows, width), bf16),
            vmem((2, tp, rows, width), bf16),
            vmem((2, rows, units), bf16),
            vmem((2, tp, rows, width), bf16),
            vmem((2, chips, rows, width), bf16),
            vmem((2, chips - 1, rows, width), bf16),
            vmem((rows, width), bf16),
            vmem((rows, width), bf16),
            vmem((rows, width), f32),
            vmem((tp, 8, rows), f32),
            dma((5, n + 1)),
            dma((messages, n)),
            dma((5, n)),
            dma((groups, n)),
            dma((5,)),
            dma((groups, 2)),
            dma((2,)),
            dma((1 + 2 * HALVES,)),
            dma((1 + 2 * HALVES, tp - 1)),
            dma((HALVES,)),
            dma((HALVES, tp - 1)),
            dma((2,)),
            dma((n * pieces, 2)),
            dma((2,)),
            dma((per * pieces, 2, chips - 1)),
            dma((HALVES,)),
            dma((HALVES,)),
            dma,
            dma((per * pieces,)),
            dma,
            dma,
            dma((12,)),
        ],
        compiler_params=pltpu.CompilerParams(
            collective_id=0, has_side_effects=True, vmem_limit_bytes=63 * 1024 * 1024
        ),
    )(
        tokens, attn_gain[None], w_low.T, w_lift, decay_bias[None], head_gain[None],
        ffn_gain[None], final_gain[None], w_query, w_key, w_value, w_out, w_gate, w_up, w_down,
    )


def solution(mesh):
    sizes = (mesh.shape["fs"], mesh.shape["tp"])
    return jax.shard_map(
        functools.partial(body, sizes),
        mesh=mesh,
        in_specs=(
            P(("grp", "fs"), "tp"),
            P(),
            P("fs", "tp"),
            P("fs", "tp"),
            P("fs", "tp"),
            P(),
            P(None, "tp"),
            P("tp"),
            P(),
            P("tp", "fs"),
            P(),
            P("fs", "tp"),
            P("fs", "tp"),
            P("tp", "fs"),
            P("tp"),
        ),
        out_specs=P(("grp", "fs"), "tp"),
        check_vma=False,
    )
```
